1024 devices in a mesh: grp: 2 (over x), fs: 16 (over z), tp: 32 (over y, core).
Axes of the slice: x: 2, y: 16, z: 16, core: 2. Of those that a mesh axis runs over, the one named last changes fastest.
The devices are a block of a 4x16x16 slice.
Arguments:
- tokens: bfloat16 [8192, 2048], P(('grp', 'fs'), 'tp'), parts along dimension 0, may hold values from -12 to 12
- gain_first: float32 [2048], P('tp'), may hold values from 0.1 to 1.9
- gate_first: float32 [2048, 5632], P('fs', 'tp'), may hold values from -0.125 to 0.125
- gate_scale_first: float32 [5632], P('tp'), may hold values from 0.5 to 2
- up_first: float32 [2048, 5632], P('fs', 'tp'), may hold values from -0.125 to 0.125
- up_scale_first: float32 [5632], P('tp'), may hold values from 0.5 to 2
- down_first: float32 [5632, 2048], P('tp', 'fs'), may hold values from -0.078125 to 0.078125
- down_scale_first: float32 [2048], P('tp'), may hold values from 0.5 to 2
- gain_second: float32 [2048], P('tp'), may hold values from 0.1 to 1.9
- gate_second: float32 [2048, 5632], P('fs', 'tp'), may hold values from -0.125 to 0.125
- gate_scale_second: float32 [5632], P('tp'), may hold values from 0.5 to 2
- up_second: float32 [2048, 5632], P('fs', 'tp'), may hold values from -0.125 to 0.125
- up_scale_second: float32 [5632], P('tp'), may hold values from 0.5 to 2
- down_second: float32 [5632, 2048], P('tp', 'fs'), may hold values from -0.078125 to 0.078125
- down_scale_second: float32 [2048], P('tp'), may hold values from 0.5 to 2
Outputs:
- stream_out: bfloat16 [8192, 2048], P(('grp', 'fs'), 'tp'), parts along dimension 0
The draws below stay inside these ranges and needn't reach their ends.
There are 2 independent parts, one for each index of `grp`. The reference program is written for one: setup_inputs(seed, part) draws one part's arguments, and reference() takes and returns one part's arrays. A program takes and returns all parts, laid end to end along the dimension named above; an argument that names none is the same for every part. Nothing has to cross between parts.
All inputs are finite; a program needn't handle non-finite values.
Results may differ from the reference program's by a relative error of at most 0.028.
Values may be sent and summed in bfloat16 or wider, within the bound.
No kernel may reach another device: no remote copies, remote signals or barrier semaphores. Data moves between devices by JAX's collectives and lax.ppermute only.
A program may use at most 32 MiB of HBM per device.

```python
import math
import jax
import jax.numpy as jnp
from jax import lax

D = 2048
FF = 5632
TOKENS = 4096
N_TP = 32


def draw_tokens(key, part):
    keys = jax.random.split(key, 7)
    column = jnp.arange(D, dtype=jnp.float32)
    place = (column + 0.5) * (2.0 / D) - 1.0
    flip = jnp.where(jax.random.uniform(keys[0], (TOKENS, 1), jnp.float32) < 0.5, -1.0, 1.0)
    tilt = flip * jax.random.uniform(keys[1], (TOKENS, 1), jnp.float32, 0.6, 1.0)
    rough = jnp.exp(jax.random.uniform(keys[2], (1, D), jnp.float32, -0.7, 0.7))
    dense = jnp.exp(tilt * place[None, :] * math.log(2.0)) * rough
    share = jnp.exp(jax.random.uniform(keys[3], (TOKENS, 1), jnp.float32, math.log(0.02), 0.0))
    center = jax.random.uniform(keys[4], (TOKENS, 1), jnp.float32, 0.0, 1.0) * D
    width = jnp.exp(jax.random.uniform(keys[5], (TOKENS, 1), jnp.float32, 0.0, math.log(3.0)))
    distance = jnp.abs(column[None, :] - center)
    distance = jnp.minimum(distance, D - distance)
    band = 4.0 * jnp.exp(-0.5 * jnp.square(distance / width))
    amplitude = share * dense + band
    values = jax.random.normal(keys[6], (TOKENS, D), jnp.float32) * amplitude
    return jnp.clip(values, -12.0, 12.0).astype(jnp.bfloat16)


def shard_levels(stream_key, dims, cuts, smallest, top_value):
    factor_of = 1.0
    for dim, parts in cuts:
        draws = jax.random.uniform(jax.random.fold_in(jax.random.fold_in(stream_key, 6), dim), (parts,), jnp.float32, smallest / len(cuts), top_value / len(cuts))
        factor_of = factor_of * jnp.repeat(jnp.exp(draws), dims[dim] // parts).reshape((-1,) + (1,) * (len(dims) - 1 - dim))
    return factor_of


def gaussian(stream_key, dims, spread, reach, shards=(), held_as=jnp.bfloat16):
    entries = jax.random.normal(stream_key, dims, jnp.float32) * spread
    if len(shards) > 0:
        entries = shard_levels(stream_key, dims, shards, -0.22, 0.18) * entries
    return jnp.clip(entries, min=-reach, max=reach).astype(held_as)


def setup_inputs(seed: int = 0, part: int = 0) -> dict:
    streams_of = jax.random.split(jax.random.key(seed), 16)
    own_keys = jax.random.split(jax.random.fold_in(streams_of[15], part), 16)
    return {
        "tokens": draw_tokens(jax.random.fold_in(jax.random.fold_in(streams_of[15], part), 71), part),
        "gain_first": jnp.clip(1.0 + 0.18 * jax.random.normal(streams_of[1], (D,), jnp.float32), 0.1, 1.9),
        "gate_first": gaussian(streams_of[2], (D, FF), D ** -0.5, 0.125, ((0, 16), (1, 32)), jnp.float32),
        "gate_scale_first": jnp.clip(jnp.exp(math.log(2.0) - 1.3862944 * jax.random.uniform(streams_of[3], (FF,), jnp.float32) ** shard_levels(streams_of[3], (FF,), ((0, 32),), -0.2, 0.2)), 0.5, 2.0),
        "up_first": gaussian(streams_of[4], (D, FF), D ** -0.5, 0.125, ((0, 16), (1, 32)), jnp.float32),
        "up_scale_first": jnp.clip(jnp.exp(math.log(2.0) - 1.3862944 * jax.random.uniform(streams_of[5], (FF,), jnp.float32) ** shard_levels(streams_of[5], (FF,), ((0, 32),), -0.2, 0.2)), 0.5, 2.0),
        "down_first": gaussian(streams_of[6], (FF, D), FF ** -0.5, 0.078125, ((0, 32), (1, 16)), jnp.float32),
        "down_scale_first": jnp.clip(jnp.exp(math.log(2.0) - 1.3862944 * jax.random.uniform(streams_of[7], (D,), jnp.float32) ** shard_levels(streams_of[7], (D,), ((0, 32),), -0.2, 0.2)), 0.5, 2.0),
        "gain_second": jnp.clip(1.0 + 0.18 * jax.random.normal(streams_of[8], (D,), jnp.float32), 0.1, 1.9),
        "gate_second": gaussian(streams_of[9], (D, FF), D ** -0.5, 0.125, ((0, 16), (1, 32)), jnp.float32),
        "gate_scale_second": jnp.clip(jnp.exp(math.log(2.0) - 1.3862944 * jax.random.uniform(streams_of[10], (FF,), jnp.float32) ** shard_levels(streams_of[10], (FF,), ((0, 32),), -0.2, 0.2)), 0.5, 2.0),
        "up_second": gaussian(streams_of[11], (D, FF), D ** -0.5, 0.125, ((0, 16), (1, 32)), jnp.float32),
        "up_scale_second": jnp.clip(jnp.exp(math.log(2.0) - 1.3862944 * jax.random.uniform(streams_of[12], (FF,), jnp.float32) ** shard_levels(streams_of[12], (FF,), ((0, 32),), -0.2, 0.2)), 0.5, 2.0),
        "down_second": gaussian(streams_of[13], (FF, D), FF ** -0.5, 0.078125, ((0, 32), (1, 16)), jnp.float32),
        "down_scale_second": jnp.clip(jnp.exp(math.log(2.0) - 1.3862944 * jax.random.uniform(streams_of[14], (D,), jnp.float32) ** shard_levels(streams_of[14], (D,), ((0, 32),), -0.2, 0.2)), 0.5, 2.0),
    }


epsilon = 1e-06

def down_total(hidden, down_bf16):
    block = FF // N_TP
    hidden_blocks = hidden.reshape(TOKENS, N_TP, block).transpose(1, 0, 2)
    weight_blocks = down_bf16.reshape(N_TP, block, D)

    def step(total, pair):
        partial_value = jnp.dot(pair[0], pair[1], preferred_element_type=jnp.float32).astype(jnp.bfloat16)
        partial_value = lax.optimization_barrier(partial_value)
        return (total + partial_value.astype(jnp.float32), None)
    total, _ = lax.scan(step, jnp.zeros((TOKENS, D), jnp.float32), (hidden_blocks, weight_blocks))
    return total

def block_apply(stream, gain, gate_w, gate_s, up_w, up_s, down_w, down_s):
    values = stream.astype(jnp.float32)
    mean_sq = lax.optimization_barrier(jnp.mean(values * values, axis=1, keepdims=True))
    normed = (values * lax.rsqrt(mean_sq + epsilon) * gain).astype(jnp.bfloat16)
    gate = jnp.dot(normed, gate_w.astype(jnp.bfloat16), preferred_element_type=jnp.float32) * gate_s
    up = jnp.dot(normed, up_w.astype(jnp.bfloat16), preferred_element_type=jnp.float32) * up_s
    hidden = (jax.nn.silu(gate) * up).astype(jnp.bfloat16)
    total = down_total(hidden, down_w.astype(jnp.bfloat16)) * down_s
    return (values + 0.5 * total).astype(jnp.bfloat16)

def reference(tokens, gain_first, gate_first, gate_scale_first, up_first, up_scale_first, down_first, down_scale_first, gain_second, gate_second, gate_scale_second, up_second, up_scale_second, down_second, down_scale_second):
    middle = block_apply(tokens, gain_first, gate_first, gate_scale_first, up_first, up_scale_first, down_first, down_scale_first)
    return block_apply(middle, gain_second, gate_second, gate_scale_second, up_second, up_scale_second, down_second, down_scale_second)
```

```python
import functools

import jax
import jax.numpy as jnp
from jax import lax
from jax.experimental import pallas as pl
from jax.experimental.pallas import tpu as pltpu
from jax.sharding import Mesh, PartitionSpec as P

epsilon = 1e-06
BF = jnp.bfloat16
F32 = jnp.float32
CORES = 2
UP = 2.0**18
SWAP = [(0, 1), (1, 0)]


def split3(v):
    hi = lax.reduce_precision(v, 8, 7)
    mid = lax.reduce_precision(v - hi, 8, 7)
    lo = v - hi - mid
    return jnp.stack([hi, mid, lo]).astype(BF)


def own_rows(gate, up, down):
    return jnp.concatenate([gate.T, up.T, down], axis=0)


def ffn_kernel(hid, width, s_ref, g_ref, sc_ref, own_ref, sib_ref, out_ref, h_ref, hd_ref):
    chunks = own_ref.shape[0]
    lane = own_ref.shape[2]
    gains = jnp.transpose(g_ref[...])
    total = jnp.zeros((lane, s_ref.shape[1]), F32)
    for z in range(chunks):
        v = s_ref[pl.ds(z * lane, lane), :].astype(F32)
        total = total + v * v
    r = lax.rsqrt(jnp.sum(total, axis=0, keepdims=True) / width + epsilon)
    for z in range(chunks):
        v = s_ref[pl.ds(z * lane, lane), :].astype(F32)
        h_ref[pl.ds(z * lane, lane), :] = (v * r * gains[:, z : z + 1]).astype(BF)
    scales = jnp.transpose(sc_ref[...])
    for k, w in enumerate((own_ref, sib_ref)):
        acc = jnp.zeros((2 * hid, s_ref.shape[1]), F32)
        for z in range(0, chunks, 2):
            lhs = jnp.concatenate([w[z, : 2 * hid, :], w[z + 1, : 2 * hid, :]], axis=1)
            acc = acc + jnp.dot(
                lhs, h_ref[pl.ds(z * lane, 2 * lane), :], preferred_element_type=F32
            )
        gate = acc[:hid] * scales[:hid, 2 * k : 2 * k + 1]
        up = acc[hid:] * scales[:hid, 2 * k + 1 : 2 * k + 2]
        hd_ref[pl.ds(k * hid, hid), :] = (gate / (1.0 + jnp.exp(-gate)) * up).astype(BF)
    hidden = hd_ref[...]
    for z in range(chunks):
        lhs = jnp.concatenate([own_ref[z, 2 * hid :, :], sib_ref[z, 2 * hid :, :]], axis=0)
        part = lax.dot_general(
            lhs, hidden, (((0,), (0,)), ((), ())), preferred_element_type=F32
        )
        out_ref[pl.ds(z * lane, lane), :] = part.astype(BF)


def ffn(s, gain, scales, own, sib, width):
    hid = own.shape[1] // 3
    vmem = pl.BlockSpec(memory_space=pltpu.VMEM)
    tokens = s.shape[1]
    rows = own.shape[0] * own.shape[2]
    flops = 2 * 3 * 2 * hid * rows * tokens
    return pl.pallas_call(
        functools.partial(ffn_kernel, hid, float(width)),
        out_shape=jax.ShapeDtypeStruct((rows, tokens), BF),
        in_specs=[vmem] * 5,
        out_specs=vmem,
        scratch_shapes=[pltpu.VMEM((rows, tokens), BF), pltpu.VMEM((2 * hid, tokens), BF)],
        cost_estimate=pl.CostEstimate(
            flops=flops, bytes_accessed=4 * own.size, transcendentals=2 * hid * tokens
        ),
    )(s, gain, scales, own, sib)


def scale_rows(own, sib):
    rows = jnp.concatenate([own, sib], axis=0)
    return jnp.pad(rows, ((0, 8 - rows.shape[0]), (0, -rows.shape[1] % 128)))


def body(
    tokens,
    gain_1,
    gate_1,
    gate_s1,
    up_1,
    up_s1,
    down_1,
    down_s1,
    gain_2,
    gate_2,
    gate_s2,
    up_2,
    up_s2,
    down_2,
    down_s2,
):
    ny = lax.axis_size("y")
    peers = ny * CORES
    mine, feats = tokens.shape
    half = mine // CORES
    width = feats * peers
    y = lax.axis_index("y")
    core = lax.axis_index("c")

    own_2 = own_rows(gate_2, up_2, down_2).astype(BF)
    own_2 = lax.all_gather(own_2, "fs", axis=0)

    st = tokens.T.reshape(feats, CORES, half).transpose(1, 0, 2)
    vecs = jnp.concatenate([split3(gain_1), split3(gain_2)], axis=1)
    more = jnp.concatenate([split3(down_s1), split3(down_s2)], axis=1)
    extra = jnp.concatenate([vecs, more, jnp.zeros((2, vecs.shape[1]), BF)], axis=0)
    extra = jnp.pad(extra, ((0, 0), (0, half - extra.shape[1])))
    sent = jnp.concatenate([st, jnp.broadcast_to(extra[None], (CORES, *extra.shape))], axis=1)
    sent = jnp.broadcast_to(sent[None], (ny, *sent.shape)).reshape(peers, *sent.shape[1:])
    got = lax.all_to_all(sent, ("y", "c"), 0, 0, tiled=True)

    scales = jnp.stack([gate_s1, up_s1, gate_s2, up_s2])
    scales_sib = lax.ppermute(scales, "c", SWAP)

    own_1 = own_rows(gate_1, up_1, down_1).astype(BF)
    own_1 = (own_1.astype(F32) * UP).astype(jnp.float16)
    own_1 = lax.all_gather(own_1, "fs", axis=0)
    own_1 = (own_1.astype(F32) * (1.0 / UP)).astype(BF)
    sib_1 = lax.ppermute(own_1, "c", SWAP)
    sib_2 = lax.ppermute(own_2, "c", SWAP)

    s = got[:, :feats].reshape(width, half)
    vec = got[:, feats : feats + 3, : 2 * feats].astype(F32).sum(axis=1)
    more = got[:, feats + 3 : feats + 6, : 2 * feats].astype(F32).sum(axis=1)
    gains_1 = vec[:, :feats].reshape(-1, half)
    gains_2 = vec[:, feats:].reshape(-1, half)
    ds_1 = more[:, :feats].reshape(ny, -1)

    part = ffn(s, gains_1, scale_rows(scales[:2], scales_sib[:2]), own_1, sib_1, width)
    chip = feats * CORES
    arrived = lax.all_to_all(part.reshape(ny, chip, half), "y", 0, 0, tiled=True)
    summed = arrived.astype(F32).sum(axis=0)
    resid = lax.dynamic_slice_in_dim(s, y * chip, chip, 0).astype(F32)
    ds = lax.dynamic_index_in_dim(ds_1, y, 0, keepdims=False)
    middle = (resid + 0.5 * summed * ds[:, None]).astype(BF)

    there = lax.dynamic_slice_in_dim(middle, (1 - core) * feats, feats, 0)
    here = lax.dynamic_slice_in_dim(middle, core * feats, feats, 0)
    other = lax.ppermute(there, "c", SWAP)
    s2 = lax.all_gather(middle, "y", axis=0, tiled=True)

    part = ffn(s2, gains_2, scale_rows(scales[2:], scales_sib[2:]), own_2, sib_2, width)
    arrived = lax.all_to_all(part.reshape(peers, feats, half), ("y", "c"), 0, 0, tiled=True)
    summed = arrived.reshape(ny, CORES, feats, half).astype(F32).sum(axis=0)
    both = jnp.where(core == 0, jnp.stack([here, other]), jnp.stack([other, here]))
    out = (both.astype(F32) + 0.5 * summed * down_s2[None, :, None]).astype(BF)
    return out.transpose(0, 2, 1).reshape(mine, feats)


def solution(mesh):
    sizes = mesh.shape
    wide = Mesh(
        mesh.devices.reshape(sizes["grp"], sizes["fs"], sizes["tp"] // CORES, CORES),
        ("grp", "fs", "y", "c"),
    )
    tp = ("y", "c")
    block = (P(tp), P("fs", tp), P(tp), P("fs", tp), P(tp), P(tp, "fs"), P(tp))
    rows = P(("grp", "fs"), tp)
    return jax.shard_map(
        body, mesh=wide, in_specs=(rows, *block, *block), out_specs=rows, check_vma=False
    )
```

```python
import functools

import jax
import jax.numpy as jnp
from jax import lax
from jax.experimental import pallas as pl
from jax.experimental.pallas import tpu as pltpu
from jax.sharding import Mesh, PartitionSpec as P

epsilon = 1e-06
BF = jnp.bfloat16
F32 = jnp.float32
CORES = 2
SIDE = 4
LANE = 128
EXTRA = 32
UP = 2.0**18
SWAP = [(0, 1), (1, 0)]
VMEM = pl.BlockSpec(memory_space=pltpu.VMEM)


def split3(v):
    hi = v.astype(BF).astype(F32)
    mid = (v - hi).astype(BF).astype(F32)
    return hi, mid, v - hi - mid


def wide_row(a):
    if a.shape[1] == LANE:
        return a
    fill = jnp.zeros((1, LANE - a.shape[1]), F32)
    return jnp.concatenate([a, fill], axis=1)


def prep_kernel(t_ref, g1, g2, d1, d2, s1, s2, s3, s4, out_ref, ext):
    peers, rows, half = out_ref.shape
    feats = t_ref.shape[0]
    ext[...] = jnp.zeros_like(ext)
    for k, (a, b) in enumerate(((g1, g2), (d1, d2))):
        for p, (u, v) in enumerate(zip(split3(a[...]), split3(b[...]))):
            ext[3 * k + p : 3 * k + p + 1, :] = wide_row(jnp.concatenate([u, v], axis=1))
    for j, ref in enumerate((s1, s2, s3, s4)):
        for p, u in enumerate(split3(ref[...])):
            at = 8 + 8 * p + 2 * j
            ext[at : at + 1, :] = u[:, :LANE]
            ext[at + 1 : at + 2, :] = wide_row(u[:, LANE:])
    tail = ext[...].astype(BF)
    for k in range(peers):
        c = k % CORES
        out_ref[k, :feats, :] = t_ref[:, c * half : (c + 1) * half]
        out_ref[k, feats:, :] = tail


def vec_column(got, peer, which, feats, col, size):
    rows = got[peer, feats + 8 : feats + EXTRA, :].astype(F32)
    rows = rows[0:8] + rows[8:16] + rows[16:24]
    turned = jnp.transpose(rows)
    cols = []
    for w in which:
        a = turned[:, 2 * w : 2 * w + 1]
        b = turned[: size - LANE, 2 * w + 1 : 2 * w + 2]
        cols.append(jnp.concatenate([a, b], axis=0))
    return cols


def ffn_kernel(hid, block, s_ref, got, own_ref, sib_ref, out_ref, h_ref, hd_ref, g_ref):
    peers = got.shape[0]
    feats = got.shape[1] - EXTRA
    tokens = got.shape[2]
    chunks, _, lane = own_ref.shape
    width = feats * peers
    me = lax.axis_index("y") * CORES + lax.axis_index("c")
    sib = lax.axis_index("y") * CORES + 1 - lax.axis_index("c")
    for p in range(peers):
        rows = got[p, feats : feats + 8, :].astype(F32)
        g_ref[p : p + 1, :] = rows[0:1] + rows[1:2] + rows[2:3]
    gains = jnp.transpose(g_ref[...])
    gains = gains[:feats] if block == 0 else gains[feats : 2 * feats]

    def piece(p):
        if block == 0:
            return got[p, :feats, :].astype(F32)
        return s_ref[pl.ds(p * feats, feats), :].astype(F32)

    total = jnp.zeros((feats, tokens), F32)
    for p in range(peers):
        v = piece(p)
        total = total + v * v
    r = lax.rsqrt(jnp.sum(total, axis=0, keepdims=True) / float(width) + epsilon)
    for p in range(peers):
        h_ref[pl.ds(p * feats, feats), :] = (piece(p) * r * gains[:, p : p + 1]).astype(BF)
    for k, (w, peer) in enumerate(((own_ref, me), (sib_ref, sib))):
        sg, su = vec_column(got, peer, (2 * block, 2 * block + 1), feats, block, hid)
        acc = jnp.zeros((2 * hid, tokens), F32)
        for z in range(0, chunks, 2):
            lhs = jnp.concatenate([w[z, : 2 * hid, :], w[z + 1, : 2 * hid, :]], axis=1)
            acc = acc + jnp.dot(
                lhs, h_ref[pl.ds(z * lane, 2 * lane), :], preferred_element_type=F32
            )
        gate = acc[:hid] * sg
        up = acc[hid:] * su
        hd_ref[pl.ds(k * hid, hid), :] = (gate / (1.0 + jnp.exp(-gate)) * up).astype(BF)
    hidden = hd_ref[...]
    for z in range(chunks):
        lhs = jnp.concatenate([own_ref[z, 2 * hid :, :], sib_ref[z, 2 * hid :, :]], axis=0)
        part = lax.dot_general(
            lhs, hidden, (((0,), (0,)), ((), ())), preferred_element_type=F32
        )
        out_ref[z % SIDE, z // SIDE] = part.astype(BF)


def chip_column(got, y, block, feats):
    cols = []
    for c in range(CORES):
        rows = got[y * CORES + c, feats : feats + 8, :].astype(F32)
        row = rows[3:4] + rows[4:5] + rows[5:6]
        turned = jnp.transpose(jnp.broadcast_to(row, (8, LANE)))
        cols.append(turned[block * feats : (block + 1) * feats, 0:1])
    return jnp.concatenate(cols, axis=0)


def close_kernel(block, sums, got, mid_ref, out_ref):
    feats = got.shape[1] - EXTRA
    y = lax.axis_index("y")
    total = sums[0].astype(F32)
    for k in range(1, sums.shape[0]):
        total = total + sums[k].astype(F32)
    if block == 0:
        resid = jnp.concatenate([got[y * CORES + c, :feats, :] for c in range(CORES)], axis=0)
    else:
        resid = mid_ref[...]
    scale = chip_column(got, y, block, feats)
    out_ref[...] = (resid.astype(F32) + 0.5 * total * scale).astype(BF)


def partial_kernel(got, out_ref):
    total = got[0].astype(F32)
    for k in range(1, got.shape[0]):
        total = total + got[k].astype(F32)
    out_ref[...] = total.astype(BF)


def call(kernel, out, args, scratch=(), flops=1000, limit=4 << 20):
    return pl.pallas_call(
        kernel,
        out_shape=out,
        in_specs=[VMEM] * len(args),
        out_specs=VMEM,
        scratch_shapes=list(scratch),
        compiler_params=pltpu.CompilerParams(vmem_limit_bytes=limit),
        cost_estimate=pl.CostEstimate(flops=flops, bytes_accessed=1 << 20, transcendentals=0),
    )(*args)


def own_rows(gate, up, down):
    return jnp.concatenate([gate.T, up.T, down], axis=0)


def body(
    tokens,
    gain_1,
    gate_1,
    gate_s1,
    up_1,
    up_s1,
    down_1,
    down_s1,
    gain_2,
    gate_2,
    gate_s2,
    up_2,
    up_s2,
    down_2,
    down_s2,
):
    ny = lax.axis_size("y")
    peers = ny * CORES
    mine, feats = tokens.shape
    half = mine // CORES
    chip = feats * CORES
    hid = gate_1.shape[1]
    near = [[SIDE * i + j for j in range(SIDE)] for i in range(ny // SIDE)]
    far = [[j + SIDE * i for i in range(ny // SIDE)] for j in range(SIDE)]

    vecs = [v[None] for v in (gain_1, gain_2, down_s1, down_s2, gate_s1, up_s1, gate_s2, up_s2)]
    sent = call(
        prep_kernel,
        jax.ShapeDtypeStruct((peers, feats + EXTRA, half), BF),
        (tokens.T, *vecs),
        [pltpu.VMEM((EXTRA, LANE), F32)],
    )
    got = lax.all_to_all(sent, ("y", "c"), 0, 0, tiled=True)

    own_2 = own_rows(gate_2, up_2, down_2).astype(BF)
    own_2 = lax.all_gather(own_2, "fs", axis=0)

    own_1 = own_rows(gate_1, up_1, down_1).astype(BF)
    own_1 = (own_1.astype(F32) * UP).astype(jnp.float16)
    own_1 = lax.all_gather(own_1, "fs", axis=0)
    own_1, got = lax.optimization_barrier((own_1, got))
    own_1 = (own_1.astype(F32) * (1.0 / UP)).astype(BF)
    sib_1 = lax.ppermute(own_1, "c", SWAP)

    def ffn(block, s, own, sib):
        return call(
            functools.partial(ffn_kernel, hid, block),
            jax.ShapeDtypeStruct((SIDE, ny // SIDE, chip, half), BF),
            (s, got, own, sib),
            [
                pltpu.VMEM((peers * feats, half), BF),
                pltpu.VMEM((CORES * hid, half), BF),
                pltpu.VMEM((peers, LANE), F32),
            ],
            flops=12 * hid * peers * feats * half,
            limit=16 << 20,
        )

    def reduced(block, part, mid):
        step = lax.all_to_all(part, "y", 0, 0, axis_index_groups=near, tiled=True)
        step = call(partial_kernel, jax.ShapeDtypeStruct(step.shape[1:], BF), (step,))
        step = lax.all_to_all(step, "y", 0, 0, axis_index_groups=far, tiled=True)
        return call(
            functools.partial(close_kernel, block),
            jax.ShapeDtypeStruct((chip, half), BF),
            (step, got, mid),
        )

    middle = reduced(0, ffn(0, gain_1[None], own_1, sib_1), gain_1[None])
    own_2, middle = lax.optimization_barrier((own_2, middle))
    sib_2 = lax.ppermute(own_2, "c", SWAP)
    whole = lax.all_gather(middle, "y", axis=0, tiled=True)
    last = reduced(1, ffn(1, whole, own_2, sib_2), middle)

    core = lax.axis_index("c")
    there = lax.dynamic_slice_in_dim(last, (1 - core) * feats, feats, 0)
    here = lax.dynamic_slice_in_dim(last, core * feats, feats, 0)
    other = lax.ppermute(there, "c", SWAP)
    first = core == 0
    both = [jnp.where(first, here, other), jnp.where(first, other, here)]
    return jnp.concatenate(both, axis=1).T


def solution(mesh):
    sizes = mesh.shape
    wide = Mesh(
        mesh.devices.reshape(sizes["grp"], sizes["fs"], sizes["tp"] // CORES, CORES),
        ("grp", "fs", "y", "c"),
    )
    tp = ("y", "c")
    block = (P(tp), P("fs", tp), P(tp), P("fs", tp), P(tp), P(tp, "fs"), P(tp))
    rows = P(("grp", "fs"), tp)
    return jax.shard_map(
        body, mesh=wide, in_specs=(rows, *block, *block), out_specs=rows, check_vma=False
    )
```

```python
import functools

import jax
import jax.numpy as jnp
from jax import lax
from jax.experimental import pallas as pl
from jax.experimental.pallas import tpu as pltpu
from jax.sharding import Mesh, PartitionSpec as P

epsilon = 1e-06
BF = jnp.bfloat16
F32 = jnp.float32
CORES = 2
SIDE = 4
LANE = 128
EXTRA = 32
UP = 2.0**18
SWAP = [(0, 1), (1, 0)]
VMEM = pl.BlockSpec(memory_space=pltpu.VMEM)


def split3(v):
    hi = v.astype(BF).astype(F32)
    mid = (v - hi).astype(BF).astype(F32)
    return hi, mid, v - hi - mid


def wide_row(a):
    if a.shape[1] == LANE:
        return a
    fill = jnp.zeros((1, LANE - a.shape[1]), F32)
    return jnp.concatenate([a, fill], axis=1)


def prep_kernel(t_hbm, *refs):
    count = 8
    sources, out_ref = refs[:count], refs[count]
    t_ref, held, ext, sems = refs[count + 1], refs[count + 2 : 2 * count + 2], *refs[-2:]
    peers, rows, half = out_ref.shape
    feats = t_hbm.shape[0]
    copies = [pltpu.make_async_copy(t_hbm, t_ref, sems.at[count])]
    for k in range(count):
        copies.append(pltpu.make_async_copy(sources[k], held[k], sems.at[k]))
    for copy in copies:
        copy.start()
    ext[...] = jnp.zeros_like(ext)
    for copy in copies:
        copy.wait()
    vecs = [ref[...] for ref in held]
    for k in range(2):
        for p, (u, v) in enumerate(zip(split3(vecs[2 * k]), split3(vecs[2 * k + 1]))):
            ext[3 * k + p : 3 * k + p + 1, :] = wide_row(jnp.concatenate([u, v], axis=1))
    for j in range(4):
        for p, u in enumerate(split3(vecs[4 + j])):
            at = 8 + 8 * p + 2 * j
            ext[at : at + 1, :] = u[:, :LANE]
            ext[at + 1 : at + 2, :] = wide_row(u[:, LANE:])
    tail = ext[...].astype(BF)
    for k in range(peers):
        c = k % CORES
        out_ref[k, :feats, :] = t_ref[:, c * half : (c + 1) * half]
        out_ref[k, feats:, :] = tail


def vec_column(got, peer, which, feats, col, size):
    rows = got[peer, feats + 8 : feats + EXTRA, :].astype(F32)
    rows = rows[0:8] + rows[8:16] + rows[16:24]
    turned = jnp.transpose(rows)
    cols = []
    for w in which:
        a = turned[:, 2 * w : 2 * w + 1]
        b = turned[: size - LANE, 2 * w + 1 : 2 * w + 2]
        cols.append(jnp.concatenate([a, b], axis=0))
    return cols


def ffn_kernel(hid, block, s_ref, got, own_ref, sib_ref, out_ref, h_ref, hd_ref, g_ref):
    peers = got.shape[0]
    feats = got.shape[1] - EXTRA
    tokens = got.shape[2]
    chunks, _, lane = own_ref.shape
    width = feats * peers
    me = lax.axis_index("y") * CORES + lax.axis_index("c")
    sib = lax.axis_index("y") * CORES + 1 - lax.axis_index("c")
    for p in range(peers):
        rows = got[p, feats : feats + 8, :].astype(F32)
        g_ref[p : p + 1, :] = rows[0:1] + rows[1:2] + rows[2:3]
    gains = jnp.transpose(g_ref[...])
    gains = gains[:feats] if block == 0 else gains[feats : 2 * feats]

    def piece(p):
        if block == 0:
            return got[p, :feats, :].astype(F32)
        return s_ref[pl.ds(p * feats, feats), :].astype(F32)

    total = jnp.zeros((feats, tokens), F32)
    for p in range(peers):
        v = piece(p)
        total = total + v * v
    r = lax.rsqrt(jnp.sum(total, axis=0, keepdims=True) / float(width) + epsilon)
    for p in range(peers):
        h_ref[pl.ds(p * feats, feats), :] = (piece(p) * r * gains[:, p : p + 1]).astype(BF)
    for k, (w, peer) in enumerate(((own_ref, me), (sib_ref, sib))):
        sg, su = vec_column(got, peer, (2 * block, 2 * block + 1), feats, block, hid)
        acc = jnp.zeros((2 * hid, tokens), F32)
        for z in range(0, chunks, 2):
            lhs = jnp.concatenate([w[z, : 2 * hid, :], w[z + 1, : 2 * hid, :]], axis=1)
            acc = acc + jnp.dot(
                lhs, h_ref[pl.ds(z * lane, 2 * lane), :], preferred_element_type=F32
            )
        gate = acc[:hid] * sg
        up = acc[hid:] * su
        hd_ref[pl.ds(k * hid, hid), :] = (gate / (1.0 + jnp.exp(-gate)) * up).astype(BF)
    hidden = hd_ref[...]
    for z in range(chunks):
        lhs = jnp.concatenate([own_ref[z, 2 * hid :, :], sib_ref[z, 2 * hid :, :]], axis=0)
        part = lax.dot_general(
            lhs, hidden, (((0,), (0,)), ((), ())), preferred_element_type=F32
        )
        if block == 0:
            out_ref[z % SIDE, z // SIDE] = part.astype(BF)
        else:
            out_ref[z] = part.astype(BF)


def down_column(got, peer, block, feats):
    rows = got[peer, feats : feats + 8, :].astype(F32)
    row = rows[3:4] + rows[4:5] + rows[5:6]
    turned = jnp.transpose(jnp.broadcast_to(row, (8, LANE)))
    return turned[block * feats : (block + 1) * feats, 0:1]


def middle_kernel(sums, got, mid_ref, there_ref):
    feats = got.shape[1] - EXTRA
    y = lax.axis_index("y")
    core = lax.axis_index("c")
    total = sums[0].astype(F32)
    for k in range(1, sums.shape[0]):
        total = total + sums[k].astype(F32)
    for c in range(CORES):
        peer = y * CORES + c
        resid = got[peer, :feats, :].astype(F32)
        scale = down_column(got, peer, 0, feats)
        part = total[c * feats : (c + 1) * feats]
        mid_ref[c * feats : (c + 1) * feats, :] = (resid + 0.5 * part * scale).astype(BF)
    there_ref[...] = mid_ref[pl.ds((1 - core) * feats, feats), :]


def last_kernel(sums, got, mid_ref, other_ref, out_ref):
    feats = got.shape[1] - EXTRA
    half = got.shape[2]
    core = lax.axis_index("c")
    scale = down_column(got, lax.axis_index("y") * CORES + core, 1, feats)
    here = mid_ref[pl.ds(core * feats, feats), :].astype(F32)
    other = other_ref[...].astype(F32)
    for c in range(CORES):
        total = sums[c].astype(F32)
        for k in range(CORES + c, sums.shape[0], CORES):
            total = total + sums[k].astype(F32)
        resid = jnp.where(core == c, here, other)
        out_ref[:, c * half : (c + 1) * half] = (resid + 0.5 * total * scale).astype(BF)


def partial_kernel(got, out_ref):
    total = got[0].astype(F32)
    for k in range(1, got.shape[0]):
        total = total + got[k].astype(F32)
    out_ref[...] = total.astype(BF)


def call(kernel, out, args, scratch=(), flops=1000, limit=4 << 20, space=pltpu.VMEM):
    specs = jax.tree.map(lambda _: VMEM, out)
    return pl.pallas_call(
        kernel,
        out_shape=out,
        in_specs=[pl.BlockSpec(memory_space=space)] * len(args),
        out_specs=specs,
        scratch_shapes=list(scratch),
        compiler_params=pltpu.CompilerParams(vmem_limit_bytes=limit),
        cost_estimate=pl.CostEstimate(flops=flops, bytes_accessed=1 << 20, transcendentals=0),
    )(*args)


def body(
    tokens,
    gain_1,
    gate_1,
    gate_s1,
    up_1,
    up_s1,
    down_1,
    down_s1,
    gain_2,
    gate_2,
    gate_s2,
    up_2,
    up_s2,
    down_2,
    down_s2,
):
    ny = lax.axis_size("y")
    peers = ny * CORES
    mine, feats = tokens.shape
    half = mine // CORES
    chip = feats * CORES
    hid = gate_1.shape[1]
    near = [[SIDE * i + j for j in range(SIDE)] for i in range(ny // SIDE)]
    far = [[j + SIDE * i for i in range(ny // SIDE)] for j in range(SIDE)]

    vecs = [v[None] for v in (gain_1, gain_2, down_s1, down_s2, gate_s1, up_s1, gate_s2, up_s2)]
    sent = call(
        prep_kernel,
        jax.ShapeDtypeStruct((peers, feats + EXTRA, half), BF),
        (tokens.T, *vecs),
        [
            pltpu.VMEM((feats, mine), BF),
            *(pltpu.VMEM(v.shape, F32) for v in vecs),
            pltpu.VMEM((EXTRA, LANE), F32),
            pltpu.SemaphoreType.DMA((len(vecs) + 1,)),
        ],
        limit=56 << 20,
        space=pltpu.HBM,
    )
    got = lax.all_to_all(sent, ("y", "c"), 0, 0, tiled=True)

    own = jnp.concatenate([gate_1.T, up_1.T, down_1, gate_2.T, up_2.T, down_2], axis=0)
    own = (own.astype(BF).astype(F32) * UP).astype(jnp.float16)
    own = lax.all_gather(own, "fs", axis=0)
    own, got = lax.optimization_barrier((own, got))
    both = [
        (own[:, k * 3 * hid : (k + 1) * 3 * hid].astype(F32) * (1.0 / UP)).astype(BF)
        for k in range(2)
    ]
    sib = [lax.ppermute(w, "c", SWAP) for w in both]

    def ffn(block, s, shape):
        return call(
            functools.partial(ffn_kernel, hid, block),
            jax.ShapeDtypeStruct((*shape, chip, half), BF),
            (s, got, both[block], sib[block]),
            [
                pltpu.VMEM((peers * feats, half), BF),
                pltpu.VMEM((CORES * hid, half), BF),
                pltpu.VMEM((peers, LANE), F32),
            ],
            flops=12 * hid * peers * feats * half,
            limit=16 << 20,
        )

    step = ffn(0, jnp.zeros((8, LANE), BF), (SIDE, ny // SIDE))
    step = lax.all_to_all(step, "y", 0, 0, axis_index_groups=near, tiled=True)
    step = call(partial_kernel, jax.ShapeDtypeStruct(step.shape[1:], BF), (step,))
    step = lax.all_to_all(step, "y", 0, 0, axis_index_groups=far, tiled=True)
    middle, there = call(
        middle_kernel,
        (jax.ShapeDtypeStruct((chip, half), BF), jax.ShapeDtypeStruct((feats, half), BF)),
        (step, got),
    )
    other = lax.ppermute(there, "c", SWAP)
    whole = lax.all_gather(middle, "y", axis=0, tiled=True)
    step = ffn(1, whole, (ny,)).reshape(peers, feats, half)
    step = lax.all_to_all(step, ("y", "c"), 0, 0, tiled=True)
    out = call(
        last_kernel, jax.ShapeDtypeStruct((feats, mine), BF), (step, got, middle, other)
    )
    return out.T


def solution(mesh):
    sizes = mesh.shape
    wide = Mesh(
        mesh.devices.reshape(sizes["grp"], sizes["fs"], sizes["tp"] // CORES, CORES),
        ("grp", "fs", "y", "c"),
    )
    tp = ("y", "c")
    block = (P(tp), P("fs", tp), P(tp), P("fs", tp), P(tp), P(tp, "fs"), P(tp))
    rows = P(("grp", "fs"), tp)
    return jax.shard_map(
        body, mesh=wide, in_specs=(rows, *block, *block), out_specs=rows, check_vma=False
    )
```

```python
import functools

import jax
import jax.numpy as jnp
from jax import lax
from jax.experimental import pallas as pl
from jax.experimental.pallas import tpu as pltpu
from jax.sharding import Mesh, PartitionSpec as P

epsilon = 1e-06
BF = jnp.bfloat16
F32 = jnp.float32
CORES = 2
SIDE = 4
LANE = 128
EXTRA = 32
UP = 2.0**18
SWAP = [(0, 1), (1, 0)]
VMEM = pl.BlockSpec(memory_space=pltpu.VMEM)


def split3(v):
    hi = v.astype(BF).astype(F32)
    mid = (v - hi).astype(BF).astype(F32)
    return hi, mid, v - hi - mid


def chip_index():
    return lax.axis_index("yh") * SIDE + lax.axis_index("yl")


def seat(other):
    core = lax.axis_index("c")
    return chip_index() * CORES + (1 - core if other else core)


def wide_row(a):
    if a.shape[1] == LANE:
        return a
    fill = jnp.zeros((1, LANE - a.shape[1]), F32)
    return jnp.concatenate([a, fill], axis=1)


def prep_kernel(t_hbm, *refs):
    count = 8
    sources, out_ref = refs[:count], refs[count]
    t_ref, held, ext, sems = refs[count + 1], refs[count + 2 : 2 * count + 2], *refs[-2:]
    peers, rows, half = out_ref.shape
    feats = t_hbm.shape[0]
    copies = [pltpu.make_async_copy(t_hbm, t_ref, sems.at[count])]
    for k in range(count):
        copies.append(pltpu.make_async_copy(sources[k], held[k], sems.at[k]))
    for copy in copies:
        copy.start()
    ext[...] = jnp.zeros_like(ext)
    for copy in copies:
        copy.wait()
    vecs = [ref[...] for ref in held]
    for k in range(2):
        for p, (u, v) in enumerate(zip(split3(vecs[2 * k]), split3(vecs[2 * k + 1]))):
            ext[3 * k + p : 3 * k + p + 1, :] = wide_row(jnp.concatenate([u, v], axis=1))
    for j in range(4):
        for p, u in enumerate(split3(vecs[4 + j])):
            at = 8 + 8 * p + 2 * j
            ext[at : at + 1, :] = u[:, :LANE]
            ext[at + 1 : at + 2, :] = wide_row(u[:, LANE:])
    tail = ext[...].astype(BF)
    for k in range(peers):
        c = k % CORES
        out_ref[k, :feats, :] = t_ref[:, c * half : (c + 1) * half]
        out_ref[k, feats:, :] = tail


def vec_column(got, peer, which, feats, col, size):
    rows = got[peer, feats + 8 : feats + EXTRA, :].astype(F32)
    rows = rows[0:8] + rows[8:16] + rows[16:24]
    turned = jnp.transpose(rows)
    cols = []
    for w in which:
        a = turned[:, 2 * w : 2 * w + 1]
        b = turned[: size - LANE, 2 * w + 1 : 2 * w + 2]
        cols.append(jnp.concatenate([a, b], axis=0))
    return cols


def normalize(block, s_ref, got, h_ref, g_ref):
    peers = got.shape[0]
    feats = got.shape[1] - EXTRA
    tokens = got.shape[2]
    width = feats * peers
    for p in range(peers):
        rows = got[p, feats : feats + 8, :].astype(F32)
        g_ref[p : p + 1, :] = rows[0:1] + rows[1:2] + rows[2:3]
    gains = jnp.transpose(g_ref[...])
    gains = gains[:feats] if block == 0 else gains[feats : 2 * feats]

    def piece(p):
        if block == 0:
            return got[p, :feats, :].astype(F32)
        return s_ref[pl.ds(p * feats, feats), :].astype(F32)

    total = jnp.zeros((feats, tokens), F32)
    for p in range(peers):
        v = piece(p)
        total = total + v * v
    r = lax.rsqrt(jnp.sum(total, axis=0, keepdims=True) / float(width) + epsilon)
    for p in range(peers):
        h_ref[pl.ds(p * feats, feats), :] = (piece(p) * r * gains[:, p : p + 1]).astype(BF)


def hidden_of(hid, block, w, peer, got, h_ref):
    feats = got.shape[1] - EXTRA
    chunks, _, lane = w.shape
    sg, su = vec_column(got, peer, (2 * block, 2 * block + 1), feats, block, hid)
    acc = jnp.zeros((2 * hid, got.shape[2]), F32)
    for z in range(0, chunks, 2):
        lhs = jnp.concatenate([w[z, : 2 * hid, :], w[z + 1, : 2 * hid, :]], axis=1)
        acc = acc + jnp.dot(
            lhs, h_ref[pl.ds(z * lane, 2 * lane), :], preferred_element_type=F32
        )
    gate = acc[:hid] * sg
    up = acc[hid:] * su
    return (gate / (1.0 + jnp.exp(-gate)) * up).astype(BF)


def down_blocks(hid, own_ref, sib_ref, hidden, store):
    for z in range(own_ref.shape[0]):
        rows = slice(2 * hid, 3 * hid)
        lhs = jnp.concatenate([own_ref[z, rows, :], sib_ref[z, rows, :]], axis=0)
        part = lax.dot_general(
            lhs, hidden, (((0,), (0,)), ((), ())), preferred_element_type=F32
        )
        store(z, part.astype(BF))


def first_half_kernel(hid, got, own_ref, h_ref, hd_ref, g_ref):
    normalize(0, None, got, h_ref, g_ref)
    hd_ref[...] = hidden_of(hid, 0, own_ref, seat(0), got, h_ref)


def second_half_kernel(hid, got, h_ref, hd_own, own_ref, sib_ref, out_ref, hd_ref):
    hd_ref[:hid, :] = hd_own[...]
    hd_ref[hid:, :] = hidden_of(hid, 0, sib_ref, seat(1), got, h_ref)

    def store(z, part):
        out_ref[z % SIDE, z // SIDE] = part

    down_blocks(hid, own_ref, sib_ref, hd_ref[...], store)


def second_block_kernel(hid, s_ref, got, own_ref, sib_ref, out_ref, h_ref, hd_ref, g_ref):
    feats = got.shape[1] - EXTRA
    normalize(1, s_ref, got, h_ref, g_ref)
    hd_ref[:hid, :] = hidden_of(hid, 1, own_ref, seat(0), got, h_ref)
    hd_ref[hid:, :] = hidden_of(hid, 1, sib_ref, seat(1), got, h_ref)

    def store(z, part):
        for c in range(CORES):
            out_ref[z % SIDE * CORES + c, z // SIDE] = part[c * feats : (c + 1) * feats]

    down_blocks(hid, own_ref, sib_ref, hd_ref[...], store)


def down_column(got, peer, block, feats):
    rows = got[peer, feats : feats + 8, :].astype(F32)
    row = rows[3:4] + rows[4:5] + rows[5:6]
    turned = jnp.transpose(jnp.broadcast_to(row, (8, LANE)))
    return turned[block * feats : (block + 1) * feats, 0:1]


def middle_kernel(sums, got, mid_ref, there_ref):
    feats = got.shape[1] - EXTRA
    y = chip_index()
    core = lax.axis_index("c")
    total = sums[0].astype(F32)
    for k in range(1, sums.shape[0]):
        total = total + sums[k].astype(F32)
    for c in range(CORES):
        peer = y * CORES + c
        resid = got[peer, :feats, :].astype(F32)
        scale = down_column(got, peer, 0, feats)
        part = total[c * feats : (c + 1) * feats]
        mid_ref[c * feats : (c + 1) * feats, :] = (resid + 0.5 * part * scale).astype(BF)
    there_ref[...] = mid_ref[pl.ds((1 - core) * feats, feats), :]


def last_kernel(sums, got, mid_ref, other_ref, out_ref):
    feats = got.shape[1] - EXTRA
    half = got.shape[2]
    core = lax.axis_index("c")
    scale = down_column(got, seat(0), 1, feats)
    here = mid_ref[pl.ds(core * feats, feats), :].astype(F32)
    other = other_ref[...].astype(F32)
    for c in range(CORES):
        total = sums[0, c].astype(F32)
        for k in range(1, sums.shape[0]):
            total = total + sums[k, c].astype(F32)
        resid = jnp.where(core == c, here, other)
        out_ref[:, c * half : (c + 1) * half] = (resid + 0.5 * total * scale).astype(BF)


def partial_kernel(got, out_ref):
    total = got[0].astype(F32)
    for k in range(1, got.shape[0]):
        total = total + got[k].astype(F32)
    out_ref[...] = total.astype(BF)


def last_partial_kernel(got, out_ref):
    for c in range(CORES):
        for i in range(out_ref.shape[0]):
            total = got[c, i].astype(F32)
            for k in range(CORES + c, got.shape[0], CORES):
                total = total + got[k, i].astype(F32)
            out_ref[i, c] = total.astype(BF)


def call(kernel, out, args, scratch=(), flops=1000, limit=4 << 20, space=pltpu.VMEM):
    specs = jax.tree.map(lambda _: VMEM, out)
    return pl.pallas_call(
        kernel,
        out_shape=out,
        in_specs=[pl.BlockSpec(memory_space=space)] * len(args),
        out_specs=specs,
        scratch_shapes=list(scratch),
        compiler_params=pltpu.CompilerParams(vmem_limit_bytes=limit),
        cost_estimate=pl.CostEstimate(flops=flops, bytes_accessed=1 << 20, transcendentals=0),
    )(*args)


def body(
    tokens,
    gain_1,
    gate_1,
    gate_s1,
    up_1,
    up_s1,
    down_1,
    down_s1,
    gain_2,
    gate_2,
    gate_s2,
    up_2,
    up_s2,
    down_2,
    down_s2,
):
    groups = lax.axis_size("grp")
    group = lax.axis_index("grp")
    far = lax.axis_size("yh")
    peers = far * SIDE * CORES
    mine, feats = tokens.shape
    half = mine // CORES
    chip = feats * CORES
    hid = gate_1.shape[1]

    vecs = [v[None] for v in (gain_1, gain_2, down_s1, down_s2, gate_s1, up_s1, gate_s2, up_s2)]
    sent = call(
        prep_kernel,
        jax.ShapeDtypeStruct((peers, feats + EXTRA, half), BF),
        (tokens.T, *vecs),
        [
            pltpu.VMEM((feats, mine), BF),
            *(pltpu.VMEM(v.shape, F32) for v in vecs),
            pltpu.VMEM((EXTRA, LANE), F32),
            pltpu.SemaphoreType.DMA((len(vecs) + 1,)),
        ],
        limit=56 << 20,
        space=pltpu.HBM,
    )
    got = lax.all_to_all(sent, ("yh", "yl", "c"), 0, 0, tiled=True)

    rows = 3 * hid
    share = -(-rows // (16 * groups)) * 16
    own_2 = jnp.concatenate([gate_2.T, up_2.T, down_2], axis=0)
    own_2 = jnp.pad(own_2, ((0, groups * share - rows), (0, 0)))
    own_2 = lax.dynamic_slice_in_dim(own_2, group * share, share, 0)
    own = jnp.concatenate([gate_1.T, up_1.T, down_1, own_2], axis=0)
    own = (own.astype(BF).astype(F32) * UP).astype(jnp.float16)
    own = lax.all_gather(own, "fs", axis=0)
    own, got = lax.optimization_barrier((own, got))

    def restored(w):
        return (w.astype(F32) * (1.0 / UP)).astype(BF)

    own_1 = restored(own[:, :rows])
    sib_1 = lax.ppermute(own_1, "c", SWAP)
    width = peers * feats
    h, hd = call(
        functools.partial(first_half_kernel, hid),
        (jax.ShapeDtypeStruct((width, half), BF), jax.ShapeDtypeStruct((hid, half), BF)),
        (got, own_1),
        [pltpu.VMEM((peers, LANE), F32)],
        flops=4 * hid * width * half,
        limit=16 << 20,
    )
    sib_1, h, hd = lax.optimization_barrier((sib_1, h, hd))
    step = call(
        functools.partial(second_half_kernel, hid),
        jax.ShapeDtypeStruct((SIDE, far, chip, half), BF),
        (got, h, hd, own_1, sib_1),
        [pltpu.VMEM((CORES * hid, half), BF)],
        flops=8 * hid * width * half,
        limit=16 << 20,
    )
    later, step = lax.optimization_barrier((own[:, rows:], step))
    later = restored(later)
    slices = [later] + [
        lax.ppermute(later, "grp", [(i, (i + r) % groups) for i in range(groups)])
        for r in range(1, groups)
    ]
    step = lax.all_to_all(step, "yl", 0, 0, tiled=True)
    step = call(partial_kernel, jax.ShapeDtypeStruct(step.shape[1:], BF), (step,))
    step = lax.all_to_all(step, "yh", 0, 0, tiled=True)
    slices, step = lax.optimization_barrier((slices, step))
    own_2 = jnp.zeros((later.shape[0], groups * share, LANE), BF)
    for r, w in enumerate(slices):
        at = (group + groups - r) % groups * share
        own_2 = lax.dynamic_update_slice_in_dim(own_2, w, at, 1)
    sib_2 = lax.ppermute(own_2, "c", SWAP)
    middle, there = call(
        middle_kernel,
        (jax.ShapeDtypeStruct((chip, half), BF), jax.ShapeDtypeStruct((feats, half), BF)),
        (step, got),
    )
    other = lax.ppermute(there, "c", SWAP)
    whole = lax.all_gather(middle, ("yh", "yl"), axis=0, tiled=True)
    step = call(
        functools.partial(second_block_kernel, hid),
        jax.ShapeDtypeStruct((SIDE * CORES, far, feats, half), BF),
        (whole, got, own_2, sib_2),
        [
            pltpu.VMEM((width, half), BF),
            pltpu.VMEM((CORES * hid, half), BF),
            pltpu.VMEM((peers, LANE), F32),
        ],
        flops=12 * hid * width * half,
        limit=16 << 20,
    )
    step = lax.all_to_all(step, ("yl", "c"), 0, 0, tiled=True)
    step = call(
        last_partial_kernel, jax.ShapeDtypeStruct((far, CORES, feats, half), BF), (step,)
    )
    step = lax.all_to_all(step, "yh", 0, 0, tiled=True)
    out = call(
        last_kernel, jax.ShapeDtypeStruct((feats, mine), BF), (step, got, middle, other)
    )
    return out.T


def solution(mesh):
    sizes = mesh.shape
    shape = (sizes["grp"], sizes["fs"], sizes["tp"] // CORES // SIDE, SIDE, CORES)
    wide = Mesh(mesh.devices.reshape(shape), ("grp", "fs", "yh", "yl", "c"))
    tp = ("yh", "yl", "c")
    block = (P(tp), P("fs", tp), P(tp), P("fs", tp), P(tp), P(tp, "fs"), P(tp))
    rows = P(("grp", "fs"), tp)
    return jax.shard_map(
        body, mesh=wide, in_specs=(rows, *block, *block), out_specs=rows, check_vma=False
    )
```

```python
import functools

import jax
import jax.numpy as jnp
from jax import lax
from jax.experimental import pallas as pl
from jax.experimental.pallas import tpu as pltpu
from jax.sharding import Mesh, PartitionSpec as P


epsilon = 1e-06
BF = jnp.bfloat16
F32 = jnp.float32
CORES = 2
SIDE = 4
LANE = 128
EXTRA = 32
UP = 2.0**18
SWAP = [(0, 1), (1, 0)]
VMEM = pl.BlockSpec(memory_space=pltpu.VMEM)


def split3(v):
    hi = v.astype(BF).astype(F32)
    mid = (v - hi).astype(BF).astype(F32)
    return hi, mid, v - hi - mid


def chip_index():
    return lax.axis_index("yh") * SIDE + lax.axis_index("yl")


def seat(other):
    core = lax.axis_index("c")
    return chip_index() * CORES + (1 - core if other else core)


def wide_row(a):
    if a.shape[1] == LANE:
        return a
    fill = jnp.zeros((1, LANE - a.shape[1]), F32)
    return jnp.concatenate([a, fill], axis=1)


def prep_kernel(t_hbm, *refs):
    count = 8
    sources, out_ref = refs[:count], refs[count]
    t_ref, held, ext, sems = refs[count + 1], refs[count + 2 : 2 * count + 2], *refs[-2:]
    peers, _, half = out_ref.shape
    feats = t_hbm.shape[0]
    copies = [pltpu.make_async_copy(t_hbm, t_ref, sems.at[count])]
    for k in range(count):
        copies.append(pltpu.make_async_copy(sources[k], held[k], sems.at[k]))
    for copy in copies:
        copy.start()
    ext[...] = jnp.zeros_like(ext)
    for copy in copies:
        copy.wait()
    vecs = [ref[...] for ref in held]
    for k in range(2):
        for p, (u, v) in enumerate(zip(split3(vecs[2 * k]), split3(vecs[2 * k + 1]))):
            ext[3 * k + p : 3 * k + p + 1, :] = wide_row(jnp.concatenate([u, v], axis=1))
    for j in range(4):
        for p, u in enumerate(split3(vecs[4 + j])):
            at = 8 + 8 * p + 2 * j
            ext[at : at + 1, :] = u[:, :LANE]
            ext[at + 1 : at + 2, :] = wide_row(u[:, LANE:])
    tail = ext[...].astype(BF)
    for k in range(peers):
        c = k % CORES
        out_ref[k, :feats, :] = t_ref[:, c * half : (c + 1) * half]
        out_ref[k, feats:, :] = tail


def vec_column(got, peer, which, feats, size):
    rows = got[peer, feats + 8 : feats + EXTRA, :].astype(F32)
    rows = rows[0:8] + rows[8:16] + rows[16:24]
    turned = jnp.transpose(rows)
    cols = []
    for w in which:
        a = turned[:, 2 * w : 2 * w + 1]
        b = turned[: size - LANE, 2 * w + 1 : 2 * w + 2]
        cols.append(jnp.concatenate([a, b], axis=0))
    return cols


def normalize(block, s_ref, got, h_ref, g_ref):
    peers = got.shape[0]
    feats = got.shape[1] - EXTRA
    tokens = got.shape[2]
    width = feats * peers
    for p in range(peers):
        rows = got[p, feats : feats + 8, :].astype(F32)
        g_ref[p : p + 1, :] = rows[0:1] + rows[1:2] + rows[2:3]
    gains = jnp.transpose(g_ref[...])
    gains = gains[:feats] if block == 0 else gains[feats : 2 * feats]

    def piece(p):
        if block == 0:
            return got[p, :feats, :].astype(F32)
        return s_ref[pl.ds(p * feats, feats), :].astype(F32)

    total = jnp.zeros((feats, tokens), F32)
    for p in range(peers):
        v = piece(p)
        total = total + v * v
    r = lax.rsqrt(jnp.sum(total, axis=0, keepdims=True) / float(width) + epsilon)
    for p in range(peers):
        h_ref[pl.ds(p * feats, feats), :] = (piece(p) * r * gains[:, p : p + 1]).astype(BF)


def hidden_of(hid, block, w, peer, got, h_ref):
    feats = got.shape[1] - EXTRA
    chunks, _, lane = w.shape
    sg, su = vec_column(got, peer, (2 * block, 2 * block + 1), feats, hid)
    acc = jnp.zeros((2 * hid, got.shape[2]), F32)
    for z in range(0, chunks, 2):
        lhs = jnp.concatenate([w[z, : 2 * hid, :], w[z + 1, : 2 * hid, :]], axis=1)
        acc = acc + jnp.dot(
            lhs, h_ref[pl.ds(z * lane, 2 * lane), :], preferred_element_type=F32
        )
    gate = acc[:hid] * sg
    up = acc[hid:] * su
    return (gate / (1.0 + jnp.exp(-gate)) * up).astype(BF)


def down_blocks(hid, own_ref, sib_ref, hidden, store):
    for z in range(own_ref.shape[0]):
        rows = slice(2 * hid, 3 * hid)
        lhs = jnp.concatenate([own_ref[z, rows, :], sib_ref[z, rows, :]], axis=0)
        part = lax.dot_general(
            lhs, hidden, (((0,), (0,)), ((), ())), preferred_element_type=F32
        )
        store(z, part.astype(BF))


def first_half_kernel(hid, got, own_ref, h_ref, hd_ref, g_ref):
    normalize(0, None, got, h_ref, g_ref)
    hd_ref[...] = hidden_of(hid, 0, own_ref, seat(0), got, h_ref)


def second_half_kernel(hid, got, h_ref, hd_own, own_ref, sib_ref, out_ref, hd_ref):
    hd_ref[:hid, :] = hd_own[...]
    hd_ref[hid:, :] = hidden_of(hid, 0, sib_ref, seat(1), got, h_ref)

    def store(z, part):
        out_ref[z % SIDE, z // SIDE] = part

    down_blocks(hid, own_ref, sib_ref, hd_ref[...], store)


def second_block_kernel(hid, s_ref, got, own_ref, sib_ref, out_ref, h_ref, hd_ref, g_ref):
    normalize(1, s_ref, got, h_ref, g_ref)
    hd_ref[:hid, :] = hidden_of(hid, 1, own_ref, seat(0), got, h_ref)
    hd_ref[hid:, :] = hidden_of(hid, 1, sib_ref, seat(1), got, h_ref)

    def store(z, part):
        out_ref[z % SIDE, z // SIDE] = part

    down_blocks(hid, own_ref, sib_ref, hd_ref[...], store)


def down_column(got, peer, block, feats):
    rows = got[peer, feats : feats + 8, :].astype(F32)
    row = rows[3:4] + rows[4:5] + rows[5:6]
    turned = jnp.transpose(jnp.broadcast_to(row, (8, LANE)))
    return turned[block * feats : (block + 1) * feats, 0:1]


def middle_kernel(sums, got, mid_ref, there_ref):
    feats = got.shape[1] - EXTRA
    y = chip_index()
    core = lax.axis_index("c")
    total = sums[0].astype(F32)
    for k in range(1, sums.shape[0]):
        total = total + sums[k].astype(F32)
    for c in range(CORES):
        peer = y * CORES + c
        resid = got[peer, :feats, :].astype(F32)
        scale = down_column(got, peer, 0, feats)
        part = total[c * feats : (c + 1) * feats]
        mid_ref[c * feats : (c + 1) * feats, :] = (resid + 0.5 * part * scale).astype(BF)
    there_ref[...] = mid_ref[pl.ds((1 - core) * feats, feats), :]


def last_kernel(sums, got, mid_ref, other_ref, out_ref):
    feats = got.shape[1] - EXTRA
    half = got.shape[2]
    core = lax.axis_index("c")
    scale = down_column(got, seat(0), 1, feats)
    here = mid_ref[pl.ds(core * feats, feats), :].astype(F32)
    other = other_ref[...].astype(F32)
    for c in range(CORES):
        total = sums[c].astype(F32)
        for k in range(CORES + c, sums.shape[0], CORES):
            total = total + sums[k].astype(F32)
        resid = jnp.where(core == c, here, other)
        out_ref[:, c * half : (c + 1) * half] = (resid + 0.5 * total * scale).astype(BF)


def partial_kernel(got, out_ref):
    total = got[0].astype(F32)
    for k in range(1, got.shape[0]):
        total = total + got[k].astype(F32)
    out_ref[...] = total.astype(BF)


def call(kernel, out, args, scratch=(), flops=1000, limit=4 << 20, space=pltpu.VMEM):
    specs = jax.tree.map(lambda _: VMEM, out)
    return pl.pallas_call(
        kernel,
        out_shape=out,
        in_specs=[pl.BlockSpec(memory_space=space)] * len(args),
        out_specs=specs,
        scratch_shapes=list(scratch),
        compiler_params=pltpu.CompilerParams(vmem_limit_bytes=limit),
        cost_estimate=pl.CostEstimate(flops=flops, bytes_accessed=1 << 20, transcendentals=0),
    )(*args)


def blocks(
    tokens,
    gain_1,
    gate_1,
    gate_s1,
    up_1,
    up_s1,
    down_1,
    down_s1,
    gain_2,
    gate_2,
    gate_s2,
    up_2,
    up_s2,
    down_2,
    down_s2,
):
    groups = lax.axis_size("grp")
    group = lax.axis_index("grp")
    far = lax.axis_size("yh")
    peers = far * SIDE * CORES
    mine, feats = tokens.shape
    half = mine // CORES
    chip = feats * CORES
    hid = gate_1.shape[1]

    vecs = [v[None] for v in (gain_1, gain_2, down_s1, down_s2, gate_s1, up_s1, gate_s2, up_s2)]
    sent = call(
        prep_kernel,
        jax.ShapeDtypeStruct((peers, feats + EXTRA, half), BF),
        (tokens.T, *vecs),
        [
            pltpu.VMEM((feats, mine), BF),
            *(pltpu.VMEM(v.shape, F32) for v in vecs),
            pltpu.VMEM((EXTRA, LANE), F32),
            pltpu.SemaphoreType.DMA((len(vecs) + 1,)),
        ],
        limit=56 << 20,
        space=pltpu.HBM,
    )
    got = lax.all_to_all(sent, ("yh", "yl", "c"), 0, 0, tiled=True)

    rows = 3 * hid
    share = -(-rows // (16 * groups)) * 16
    own_2 = jnp.concatenate([gate_2.T, up_2.T, down_2], axis=0)
    own_2 = jnp.pad(own_2, ((0, groups * share - rows), (0, 0)))
    own_2 = lax.dynamic_slice_in_dim(own_2, group * share, share, 0)
    own = jnp.concatenate([gate_1.T, up_1.T, down_1, own_2], axis=0)
    own = (own.astype(BF).astype(F32) * UP).astype(jnp.float16)
    own = lax.all_gather(own, "fs", axis=0)
    own, got = lax.optimization_barrier((own, got))

    def restored(w):
        return (w.astype(F32) * (1.0 / UP)).astype(BF)

    own_1 = restored(own[:, :rows])
    sib_1 = lax.ppermute(own_1, "c", SWAP)
    width = peers * feats
    h, hd = call(
        functools.partial(first_half_kernel, hid),
        (jax.ShapeDtypeStruct((width, half), BF), jax.ShapeDtypeStruct((hid, half), BF)),
        (got, own_1),
        [pltpu.VMEM((peers, LANE), F32)],
        flops=4 * hid * width * half,
        limit=16 << 20,
    )
    later, h, hd = lax.optimization_barrier((own[:, rows:], h, hd))
    later = restored(later)
    slices = [later] + [
        lax.ppermute(later, "grp", [(i, (i + r) % groups) for i in range(groups)])
        for r in range(1, groups)
    ]
    later, sib_1, h, hd = lax.optimization_barrier((later, sib_1, h, hd))
    step = call(
        functools.partial(second_half_kernel, hid),
        jax.ShapeDtypeStruct((SIDE, far, chip, half), BF),
        (got, h, hd, own_1, sib_1),
        [pltpu.VMEM((CORES * hid, half), BF)],
        flops=8 * hid * width * half,
        limit=16 << 20,
    )
    step = lax.all_to_all(step, "yl", 0, 0, tiled=True)
    step = call(partial_kernel, jax.ShapeDtypeStruct(step.shape[1:], BF), (step,))
    step = lax.all_to_all(step, "yh", 0, 0, tiled=True)
    slices, step = lax.optimization_barrier((slices, step))
    own_2 = jnp.zeros((later.shape[0], groups * share, LANE), BF)
    for r, w in enumerate(slices):
        at = (group + groups - r) % groups * share
        own_2 = lax.dynamic_update_slice_in_dim(own_2, w, at, 1)
    sib_2 = lax.ppermute(own_2, "c", SWAP)
    middle, there = call(
        middle_kernel,
        (jax.ShapeDtypeStruct((chip, half), BF), jax.ShapeDtypeStruct((feats, half), BF)),
        (step, got),
    )
    other = lax.ppermute(there, "c", SWAP)
    whole = lax.all_gather(middle, ("yh", "yl"), axis=0, tiled=True)
    step = call(
        functools.partial(second_block_kernel, hid),
        jax.ShapeDtypeStruct((SIDE, far, chip, half), BF),
        (whole, got, own_2, sib_2),
        [
            pltpu.VMEM((width, half), BF),
            pltpu.VMEM((CORES * hid, half), BF),
            pltpu.VMEM((peers, LANE), F32),
        ],
        flops=12 * hid * width * half,
        limit=16 << 20,
    )
    step = lax.all_to_all(step, "yl", 0, 0, tiled=True)
    step = call(partial_kernel, jax.ShapeDtypeStruct(step.shape[1:], BF), (step,))
    step = step.reshape(far * CORES, feats, half)
    step = lax.all_to_all(step, ("yh", "c"), 0, 0, tiled=True)
    out = call(
        last_kernel, jax.ShapeDtypeStruct((feats, mine), BF), (step, got, middle, other)
    )
    return out.T


def solution(mesh):
    sizes = mesh.shape
    shape = (sizes["grp"], sizes["fs"], sizes["tp"] // CORES // SIDE, SIDE, CORES)
    wide = Mesh(mesh.devices.reshape(shape), ("grp", "fs", "yh", "yl", "c"))
    tp = ("yh", "yl", "c")
    block = (P(tp), P("fs", tp), P(tp), P("fs", tp), P(tp), P(tp, "fs"), P(tp))
    rows = P(("grp", "fs"), tp)
    return jax.shard_map(
        blocks, mesh=wide, in_specs=(rows, *block, *block), out_specs=rows, check_vma=False
    )
```

```python
import functools

import jax
import jax.numpy as jnp
from jax import lax
from jax.experimental import pallas as pl
from jax.experimental.pallas import tpu as pltpu
from jax.sharding import Mesh, PartitionSpec as P


epsilon = 1e-06
BF = jnp.bfloat16
F32 = jnp.float32
CORES = 2
SIDE = 4
LANE = 128
EXTRA = 32
UP = 2.0**18
TOP = 13.0
SWAP = [(0, 1), (1, 0)]
VMEM = pl.BlockSpec(memory_space=pltpu.VMEM)


def split3(v):
    hi = v.astype(BF).astype(F32)
    mid = (v - hi).astype(BF).astype(F32)
    return hi, mid, v - hi - mid


def chip_index():
    return lax.axis_index("yh") * SIDE + lax.axis_index("yl")


def seat(other):
    core = lax.axis_index("c")
    return chip_index() * CORES + (1 - core if other else core)


def wide_row(a):
    if a.shape[1] == LANE:
        return a
    fill = jnp.zeros((1, LANE - a.shape[1]), F32)
    return jnp.concatenate([a, fill], axis=1)


def prep_kernel(t_hbm, *refs):
    count = 8
    sources, out_ref = refs[:count], refs[count]
    t_ref, held, ext, sems = refs[count + 1], refs[count + 2 : 2 * count + 2], *refs[-2:]
    peers, _, half = out_ref.shape
    feats = t_hbm.shape[0]
    copies = [pltpu.make_async_copy(t_hbm, t_ref, sems.at[count])]
    for k in range(count):
        copies.append(pltpu.make_async_copy(sources[k], held[k], sems.at[k]))
    for copy in copies:
        copy.start()
    ext[...] = jnp.zeros_like(ext)
    for copy in copies:
        copy.wait()
    vecs = [ref[...] for ref in held]
    for k in range(2):
        for p, (u, v) in enumerate(zip(split3(vecs[2 * k]), split3(vecs[2 * k + 1]))):
            ext[3 * k + p : 3 * k + p + 1, :] = wide_row(jnp.concatenate([u, v], axis=1))
    for j in range(4):
        for p, u in enumerate(split3(vecs[4 + j])):
            at = 8 + 8 * p + 2 * j
            ext[at : at + 1, :] = u[:, :LANE]
            ext[at + 1 : at + 2, :] = wide_row(u[:, LANE:])
    tail = ext[...].astype(BF)
    for k in range(peers):
        c = k % CORES
        out_ref[k, :feats, :] = t_ref[:, c * half : (c + 1) * half]
        out_ref[k, feats:, :] = tail


def vec_column(got, peer, which, feats, size):
    rows = got[peer, feats + 8 : feats + EXTRA, :].astype(F32)
    rows = rows[0:8] + rows[8:16] + rows[16:24]
    turned = jnp.transpose(rows)
    cols = []
    for w in which:
        a = turned[:, 2 * w : 2 * w + 1]
        b = turned[: size - LANE, 2 * w + 1 : 2 * w + 2]
        cols.append(jnp.concatenate([a, b], axis=0))
    return cols


def columns(got, rows, ref):
    feats = got.shape[1] - EXTRA
    for p in range(got.shape[0]):
        v = got[p, feats : feats + 8, :].astype(F32)
        ref[p : p + 1, :] = v[rows : rows + 1] + v[rows + 1 : rows + 2] + v[rows + 2 : rows + 3]
    return jnp.transpose(ref[...])


def normalize(block, piece, got, h_ref, g_ref):
    peers = got.shape[0]
    feats = got.shape[1] - EXTRA
    tokens = got.shape[2]
    width = feats * peers
    gains = columns(got, 0, g_ref)
    gains = gains[:feats] if block == 0 else gains[feats : 2 * feats]
    total = jnp.zeros((feats, tokens), F32)
    for p in range(peers):
        v = piece(p)
        total = total + v * v
    r = lax.rsqrt(jnp.sum(total, axis=0, keepdims=True) / float(width) + epsilon)
    for p in range(peers):
        h_ref[pl.ds(p * feats, feats), :] = (piece(p) * r * gains[:, p : p + 1]).astype(BF)


def hidden_of(hid, block, w, peer, got, h_ref):
    feats = got.shape[1] - EXTRA
    chunks, _, lane = w.shape
    sg, su = vec_column(got, peer, (2 * block, 2 * block + 1), feats, hid)
    acc = jnp.zeros((2 * hid, got.shape[2]), F32)
    for z in range(0, chunks, 2):
        lhs = jnp.concatenate([w[z, : 2 * hid, :], w[z + 1, : 2 * hid, :]], axis=1)
        acc = acc + jnp.dot(
            lhs, h_ref[pl.ds(z * lane, 2 * lane), :], preferred_element_type=F32
        )
    gate = acc[:hid] * sg
    up = acc[hid:] * su
    return (gate / (1.0 + jnp.exp(-gate)) * up).astype(BF)


def down_blocks(hid, own_ref, sib_ref, hidden, store):
    for z in range(own_ref.shape[0]):
        rows = slice(2 * hid, 3 * hid)
        lhs = jnp.concatenate([own_ref[z, rows, :], sib_ref[z, rows, :]], axis=0)
        part = lax.dot_general(
            lhs, hidden, (((0,), (0,)), ((), ())), preferred_element_type=F32
        )
        store(z, part.astype(BF))


def first_half_kernel(hid, got, own_ref, h_ref, hd_ref, g_ref):
    feats = got.shape[1] - EXTRA
    normalize(0, lambda p: got[p, :feats, :].astype(F32), got, h_ref, g_ref)
    hd_ref[...] = hidden_of(hid, 0, own_ref, seat(0), got, h_ref)


def second_half_kernel(hid, got, h_ref, hd_own, own_ref, sib_ref, out_ref, hd_ref):
    hd_ref[:hid, :] = hd_own[...]
    hd_ref[hid:, :] = hidden_of(hid, 0, sib_ref, seat(1), got, h_ref)

    def store(z, part):
        out_ref[z % SIDE, z // SIDE] = part

    down_blocks(hid, own_ref, sib_ref, hd_ref[...], store)


def second_block_kernel(
    hid, sums, got, own_ref, sib_ref, out_ref, mid_ref, there_ref, s_ref, h_ref, hd_ref, g_ref
):
    feats = got.shape[1] - EXTRA
    scales = columns(got, 3, g_ref)[:feats]
    for p in range(got.shape[0]):
        chip, c = divmod(p, CORES)
        part = sums[chip % SIDE, chip // SIDE, c * feats : (c + 1) * feats, :]
        mid = got[p, :feats, :].astype(F32) + 0.5 * part * scales[:, p : p + 1]
        s_ref[pl.ds(p * feats, feats), :] = mid.astype(BF)
    mine = chip_index() * CORES * feats
    mid_ref[...] = s_ref[pl.ds(mine, CORES * feats), :]
    there_ref[...] = s_ref[pl.ds(mine + (1 - lax.axis_index("c")) * feats, feats), :]
    normalize(1, lambda p: s_ref[pl.ds(p * feats, feats), :].astype(F32), got, h_ref, g_ref)
    hd_ref[:hid, :] = hidden_of(hid, 1, own_ref, seat(0), got, h_ref)
    hd_ref[hid:, :] = hidden_of(hid, 1, sib_ref, seat(1), got, h_ref)

    def store(z, part):
        out_ref[z % SIDE, z // SIDE] = part

    down_blocks(hid, own_ref, sib_ref, hd_ref[...], store)


def down_column(got, peer, block, feats):
    rows = got[peer, feats : feats + 8, :].astype(F32)
    row = rows[3:4] + rows[4:5] + rows[5:6]
    turned = jnp.transpose(jnp.broadcast_to(row, (8, LANE)))
    return turned[block * feats : (block + 1) * feats, 0:1]


def last_kernel(sums, got, mid_ref, other_ref, out_ref):
    feats = got.shape[1] - EXTRA
    half = got.shape[2]
    core = lax.axis_index("c")
    scale = down_column(got, seat(0), 1, feats)
    here = mid_ref[pl.ds(core * feats, feats), :].astype(F32)
    other = other_ref[...].astype(F32)
    for c in range(CORES):
        total = sums[c].astype(F32)
        for k in range(CORES + c, sums.shape[0], CORES):
            total = total + sums[k].astype(F32)
        resid = jnp.where(core == c, here, other)
        out_ref[:, c * half : (c + 1) * half] = (resid + 0.5 * total * scale).astype(BF)


def partial_kernel(got, out_ref):
    total = got[0].astype(F32)
    for k in range(1, got.shape[0]):
        total = total + got[k].astype(F32)
    out_ref[...] = total.astype(BF)


def scaled_kernel(got, out_ref):
    far, chip, _ = got.shape[1:]
    total = got[0].astype(F32)
    for k in range(1, got.shape[0]):
        total = total + got[k].astype(F32)
    top = jnp.max(jnp.max(jnp.abs(total), axis=0), axis=0, keepdims=True)
    power = jnp.clip(jnp.floor(jnp.log2(top)), -100.0, 120.0)
    factor = jnp.exp2(TOP - power)
    for i in range(far):
        out_ref[i * chip : (i + 1) * chip, :] = total[i] * factor
    tail = out_ref.shape[0] - far * chip
    out_ref[far * chip :, :] = jnp.broadcast_to(power, (tail, power.shape[1]))


def call(kernel, out, args, scratch=(), flops=1000, limit=4 << 20, space=pltpu.VMEM):
    specs = jax.tree.map(lambda _: VMEM, out)
    return pl.pallas_call(
        kernel,
        out_shape=out,
        in_specs=[pl.BlockSpec(memory_space=space)] * len(args),
        out_specs=specs,
        scratch_shapes=list(scratch),
        compiler_params=pltpu.CompilerParams(vmem_limit_bytes=limit),
        cost_estimate=pl.CostEstimate(flops=flops, bytes_accessed=1 << 20, transcendentals=0),
    )(*args)


def blocks(
    tokens,
    gain_1,
    gate_1,
    gate_s1,
    up_1,
    up_s1,
    down_1,
    down_s1,
    gain_2,
    gate_2,
    gate_s2,
    up_2,
    up_s2,
    down_2,
    down_s2,
):
    groups = lax.axis_size("grp")
    group = lax.axis_index("grp")
    far = lax.axis_size("yh")
    peers = far * SIDE * CORES
    mine, feats = tokens.shape
    half = mine // CORES
    chip = feats * CORES
    hid = gate_1.shape[1]

    vecs = [v[None] for v in (gain_1, gain_2, down_s1, down_s2, gate_s1, up_s1, gate_s2, up_s2)]
    sent = call(
        prep_kernel,
        jax.ShapeDtypeStruct((peers, feats + EXTRA, half), BF),
        (tokens.T, *vecs),
        [
            pltpu.VMEM((feats, mine), BF),
            *(pltpu.VMEM(v.shape, F32) for v in vecs),
            pltpu.VMEM((EXTRA, LANE), F32),
            pltpu.SemaphoreType.DMA((len(vecs) + 1,)),
        ],
        limit=56 << 20,
        space=pltpu.HBM,
    )
    got = lax.all_to_all(sent, ("yh", "yl", "c"), 0, 0, tiled=True)

    rows = 3 * hid
    share = -(-rows // (16 * groups)) * 16
    own_2 = jnp.concatenate([gate_2.T, up_2.T, down_2], axis=0)
    own_2 = jnp.pad(own_2, ((0, groups * share - rows), (0, 0)))
    own_2 = lax.dynamic_slice_in_dim(own_2, group * share, share, 0)
    own = jnp.concatenate([gate_1.T, up_1.T, down_1, own_2], axis=0)
    own = (own.astype(BF).astype(F32) * UP).astype(jnp.float16)
    own = lax.all_gather(own, "fs", axis=0)
    own, got = lax.optimization_barrier((own, got))

    def restored(w):
        return (w.astype(F32) * (1.0 / UP)).astype(BF)

    own_1 = restored(own[:, :rows])
    sib_1 = lax.ppermute(own_1, "c", SWAP)
    width = peers * feats
    h, hd = call(
        functools.partial(first_half_kernel, hid),
        (jax.ShapeDtypeStruct((width, half), BF), jax.ShapeDtypeStruct((hid, half), BF)),
        (got, own_1),
        [pltpu.VMEM((peers, LANE), F32)],
        flops=4 * hid * width * half,
        limit=16 << 20,
    )
    later, h, hd = lax.optimization_barrier((own[:, rows:], h, hd))
    later = restored(later)
    slices = [later] + [
        lax.ppermute(later, "grp", [(i, (i + r) % groups) for i in range(groups)])
        for r in range(1, groups)
    ]
    later, sib_1, h, hd = lax.optimization_barrier((later, sib_1, h, hd))
    step = call(
        functools.partial(second_half_kernel, hid),
        jax.ShapeDtypeStruct((SIDE, far, chip, half), BF),
        (got, h, hd, own_1, sib_1),
        [pltpu.VMEM((CORES * hid, half), BF)],
        flops=8 * hid * width * half,
        limit=16 << 20,
    )
    step = lax.all_to_all(step, "yl", 0, 0, tiled=True)
    size = far * chip
    step = call(scaled_kernel, jax.ShapeDtypeStruct((size + 16, half), F32), (step,))
    step = step.astype(jnp.float16)
    slices, step = lax.optimization_barrier((slices, step))
    own_2 = jnp.zeros((later.shape[0], groups * share, LANE), BF)
    for r, w in enumerate(slices):
        at = (group + groups - r) % groups * share
        own_2 = lax.dynamic_update_slice_in_dim(own_2, w, at, 1)
    sib_2 = lax.ppermute(own_2, "c", SWAP)
    shares = lax.all_gather(step, ("yh", "yl"), axis=0)
    factor = jnp.exp2(shares[:, size].astype(F32) - TOP)
    shares, factor = lax.optimization_barrier((shares, factor))
    sums = 0.0
    for k in range(far):
        part = slice(k * SIDE, (k + 1) * SIDE)
        sums = sums + shares[part, :size].astype(F32) * factor[part, None, :]
    sums = sums.reshape(SIDE, far, chip, half)
    step, middle, there = call(
        functools.partial(second_block_kernel, hid),
        (
            jax.ShapeDtypeStruct((SIDE, far, chip, half), BF),
            jax.ShapeDtypeStruct((chip, half), BF),
            jax.ShapeDtypeStruct((feats, half), BF),
        ),
        (sums, got, own_2, sib_2),
        [
            pltpu.VMEM((width, half), BF),
            pltpu.VMEM((width, half), BF),
            pltpu.VMEM((CORES * hid, half), BF),
            pltpu.VMEM((peers, LANE), F32),
        ],
        flops=12 * hid * width * half,
        limit=16 << 20,
    )
    other = lax.ppermute(there, "c", SWAP)
    step = lax.all_to_all(step, "yl", 0, 0, tiled=True)
    step = call(partial_kernel, jax.ShapeDtypeStruct(step.shape[1:], BF), (step,))
    step = step.reshape(far * CORES, feats, half)
    step = lax.all_to_all(step, ("yh", "c"), 0, 0, tiled=True)
    out = call(
        last_kernel, jax.ShapeDtypeStruct((feats, mine), BF), (step, got, middle, other)
    )
    return out.T


def solution(mesh):
    sizes = mesh.shape
    shape = (sizes["grp"], sizes["fs"], sizes["tp"] // CORES // SIDE, SIDE, CORES)
    wide = Mesh(mesh.devices.reshape(shape), ("grp", "fs", "yh", "yl", "c"))
    tp = ("yh", "yl", "c")
    block = (P(tp), P("fs", tp), P(tp), P("fs", tp), P(tp), P(tp, "fs"), P(tp))
    rows = P(("grp", "fs"), tp)
    return jax.shard_map(
        blocks, mesh=wide, in_specs=(rows, *block, *block), out_specs=rows, check_vma=False
    )
```

```python
import functools

import jax
import jax.numpy as jnp
from jax import lax
from jax.experimental import pallas as pl
from jax.experimental.pallas import tpu as pltpu
from jax.sharding import Mesh, PartitionSpec as P

epsilon = 1e-06
BF = jnp.bfloat16
F32 = jnp.float32
CORES = 2
SIDE = 4
LANE = 128
EXTRA = 32
UP = 2.0**18
TOP = 13.0
SWAP = [(0, 1), (1, 0)]
VMEM = pl.BlockSpec(memory_space=pltpu.VMEM)


def split3(v):
    hi = v.astype(BF).astype(F32)
    mid = (v - hi).astype(BF).astype(F32)
    return hi, mid, v - hi - mid


def chip_index():
    return lax.axis_index("yh") * SIDE + lax.axis_index("yl")


def seat(other):
    core = lax.axis_index("c")
    return chip_index() * CORES + (1 - core if other else core)


def wide_row(a):
    if a.shape[1] == LANE:
        return a
    fill = jnp.zeros((1, LANE - a.shape[1]), F32)
    return jnp.concatenate([a, fill], axis=1)


def prep_kernel(t_hbm, *refs):
    count = 8
    sources, out_ref = refs[:count], refs[count]
    t_ref, held, ext, sems = refs[count + 1], refs[count + 2 : 2 * count + 2], *refs[-2:]
    peers, rows, half = out_ref.shape
    feats = t_hbm.shape[0]
    copies = [pltpu.make_async_copy(t_hbm, t_ref, sems.at[count])]
    for k in range(count):
        copies.append(pltpu.make_async_copy(sources[k], held[k], sems.at[k]))
    for copy in copies:
        copy.start()
    ext[...] = jnp.zeros_like(ext)
    for copy in copies:
        copy.wait()
    vecs = [ref[...] for ref in held]
    for k in range(2):
        for p, (u, v) in enumerate(zip(split3(vecs[2 * k]), split3(vecs[2 * k + 1]))):
            ext[3 * k + p : 3 * k + p + 1, :] = wide_row(jnp.concatenate([u, v], axis=1))
    for j in range(4):
        for p, u in enumerate(split3(vecs[4 + j])):
            at = 8 + 8 * p + 2 * j
            ext[at : at + 1, :] = u[:, :LANE]
            ext[at + 1 : at + 2, :] = wide_row(u[:, LANE:])
    tail = ext[...].astype(BF)
    for k in range(peers):
        c = k % CORES
        out_ref[k, :feats, :] = t_ref[:, c * half : (c + 1) * half]
        out_ref[k, feats:, :] = tail


def vec_column(got, peer, which, feats, col, size):
    rows = got[peer, feats + 8 : feats + EXTRA, :].astype(F32)
    rows = rows[0:8] + rows[8:16] + rows[16:24]
    turned = jnp.transpose(rows)
    cols = []
    for w in which:
        a = turned[:, 2 * w : 2 * w + 1]
        b = turned[: size - LANE, 2 * w + 1 : 2 * w + 2]
        cols.append(jnp.concatenate([a, b], axis=0))
    return cols


def columns(got, rows, ref):
    feats = got.shape[1] - EXTRA
    for p in range(got.shape[0]):
        v = got[p, feats : feats + 8, :].astype(F32)
        ref[p : p + 1, :] = v[rows : rows + 1] + v[rows + 1 : rows + 2] + v[rows + 2 : rows + 3]
    return jnp.transpose(ref[...])


def normalize(block, piece, got, h_ref, g_ref):
    peers = got.shape[0]
    feats = got.shape[1] - EXTRA
    tokens = got.shape[2]
    width = feats * peers
    gains = columns(got, 0, g_ref)
    gains = gains[:feats] if block == 0 else gains[feats : 2 * feats]
    total = jnp.zeros((feats, tokens), F32)
    for p in range(peers):
        v = piece(p)
        total = total + v * v
    r = lax.rsqrt(jnp.sum(total, axis=0, keepdims=True) / float(width) + epsilon)
    for p in range(peers):
        h_ref[pl.ds(p * feats, feats), :] = (piece(p) * r * gains[:, p : p + 1]).astype(BF)


def hidden_of(hid, block, w, peer, got, h_ref):
    feats = got.shape[1] - EXTRA
    chunks, _, lane = w.shape
    sg, su = vec_column(got, peer, (2 * block, 2 * block + 1), feats, block, hid)
    acc = jnp.zeros((2 * hid, got.shape[2]), F32)
    for z in range(0, chunks, 2):
        lhs = jnp.concatenate([w[z, : 2 * hid, :], w[z + 1, : 2 * hid, :]], axis=1)
        acc = acc + jnp.dot(
            lhs, h_ref[pl.ds(z * lane, 2 * lane), :], preferred_element_type=F32
        )
    gate = acc[:hid] * sg
    up = acc[hid:] * su
    return (gate / (1.0 + jnp.exp(-gate)) * up).astype(BF)


def down_blocks(hid, own_ref, sib_ref, hidden, store):
    for z in range(own_ref.shape[0]):
        rows = slice(2 * hid, 3 * hid)
        lhs = jnp.concatenate([own_ref[z, rows, :], sib_ref[z, rows, :]], axis=0)
        part = lax.dot_general(
            lhs, hidden, (((0,), (0,)), ((), ())), preferred_element_type=F32
        )
        store(z, part.astype(BF))


def first_half_kernel(hid, got, own_ref, h_ref, hd_ref, g_ref):
    feats = got.shape[1] - EXTRA
    normalize(0, lambda p: got[p, :feats, :].astype(F32), got, h_ref, g_ref)
    hd_ref[...] = hidden_of(hid, 0, own_ref, seat(0), got, h_ref)


def second_half_kernel(hid, got, h_ref, hd_own, own_ref, sib_ref, out_ref, hd_ref):
    hd_ref[:hid, :] = hd_own[...]
    hd_ref[hid:, :] = hidden_of(hid, 0, sib_ref, seat(1), got, h_ref)

    def store(z, part):
        out_ref[z % SIDE, z // SIDE] = part

    down_blocks(hid, own_ref, sib_ref, hd_ref[...], store)


def second_block_kernel(
    hid, sums, got, own_ref, sib_ref, out_ref, mid_ref, there_ref, s_ref, h_ref, hd_ref, g_ref
):
    feats = got.shape[1] - EXTRA
    scales = columns(got, 3, g_ref)[:feats]
    for p in range(got.shape[0]):
        chip, c = divmod(p, CORES)
        part = sums[chip % SIDE, chip // SIDE, c * feats : (c + 1) * feats, :]
        mid = got[p, :feats, :].astype(F32) + 0.5 * part * scales[:, p : p + 1]
        s_ref[pl.ds(p * feats, feats), :] = mid.astype(BF)
    mine = chip_index() * CORES * feats
    mid_ref[...] = s_ref[pl.ds(mine, CORES * feats), :]
    there_ref[...] = s_ref[pl.ds(mine + (1 - lax.axis_index("c")) * feats, feats), :]
    normalize(1, lambda p: s_ref[pl.ds(p * feats, feats), :].astype(F32), got, h_ref, g_ref)
    hd_ref[:hid, :] = hidden_of(hid, 1, own_ref, seat(0), got, h_ref)
    hd_ref[hid:, :] = hidden_of(hid, 1, sib_ref, seat(1), got, h_ref)

    def store(z, part):
        out_ref[z % SIDE, z // SIDE] = part

    down_blocks(hid, own_ref, sib_ref, hd_ref[...], store)


def down_column(got, peer, block, feats):
    rows = got[peer, feats : feats + 8, :].astype(F32)
    row = rows[3:4] + rows[4:5] + rows[5:6]
    turned = jnp.transpose(jnp.broadcast_to(row, (8, LANE)))
    return turned[block * feats : (block + 1) * feats, 0:1]


def last_kernel(sums, got, mid_ref, other_ref, out_ref):
    feats = got.shape[1] - EXTRA
    half = got.shape[2]
    core = lax.axis_index("c")
    scale = down_column(got, seat(0), 1, feats)
    here = mid_ref[pl.ds(core * feats, feats), :].astype(F32)
    other = other_ref[...].astype(F32)
    for c in range(CORES):
        total = sums[c].astype(F32)
        for k in range(CORES + c, sums.shape[0], CORES):
            total = total + sums[k].astype(F32)
        resid = jnp.where(core == c, here, other)
        out_ref[:, c * half : (c + 1) * half] = (resid + 0.5 * total * scale).astype(BF)


def partial_kernel(got, out_ref):
    total = got[0].astype(F32)
    for k in range(1, got.shape[0]):
        total = total + got[k].astype(F32)
    out_ref[...] = total.astype(BF)


def scaled_kernel(got, out_ref):
    far, chip, _ = got.shape[1:]
    total = got[0].astype(F32)
    for k in range(1, got.shape[0]):
        total = total + got[k].astype(F32)
    top = jnp.max(jnp.max(jnp.abs(total), axis=0), axis=0, keepdims=True)
    power = jnp.clip(jnp.floor(jnp.log2(top)), -100.0, 120.0)
    factor = jnp.exp2(TOP - power)
    for i in range(far):
        out_ref[i * chip : (i + 1) * chip, :] = total[i] * factor
    tail = out_ref.shape[0] - far * chip
    out_ref[far * chip :, :] = jnp.broadcast_to(power, (tail, power.shape[1]))


def call(kernel, out, args, scratch=(), flops=1000, limit=4 << 20, space=pltpu.VMEM):
    specs = jax.tree.map(lambda _: VMEM, out)
    return pl.pallas_call(
        kernel,
        out_shape=out,
        in_specs=[pl.BlockSpec(memory_space=space)] * len(args),
        out_specs=specs,
        scratch_shapes=list(scratch),
        compiler_params=pltpu.CompilerParams(vmem_limit_bytes=limit),
        cost_estimate=pl.CostEstimate(flops=flops, bytes_accessed=1 << 20, transcendentals=0),
    )(*args)


def body(
    tokens,
    gain_1,
    gate_1,
    gate_s1,
    up_1,
    up_s1,
    down_1,
    down_s1,
    gain_2,
    gate_2,
    gate_s2,
    up_2,
    up_s2,
    down_2,
    down_s2,
):
    far = lax.axis_size("yh")
    peers = far * SIDE * CORES
    mine, feats = tokens.shape
    half = mine // CORES
    chip = feats * CORES
    hid = gate_1.shape[1]

    vecs = [v[None] for v in (gain_1, gain_2, down_s1, down_s2, gate_s1, up_s1, gate_s2, up_s2)]
    sent = call(
        prep_kernel,
        jax.ShapeDtypeStruct((peers, feats + EXTRA, half), BF),
        (tokens.T, *vecs),
        [
            pltpu.VMEM((feats, mine), BF),
            *(pltpu.VMEM(v.shape, F32) for v in vecs),
            pltpu.VMEM((EXTRA, LANE), F32),
            pltpu.SemaphoreType.DMA((len(vecs) + 1,)),
        ],
        limit=56 << 20,
        space=pltpu.HBM,
    )
    got = lax.all_to_all(sent, ("yh", "yl", "c"), 0, 0, tiled=True)

    rows = 3 * hid
    own = jnp.concatenate([gate_1.T, up_1.T, down_1, gate_2.T, up_2.T, down_2], axis=0)
    own = (own.astype(BF).astype(F32) * UP).astype(jnp.float16)
    own = lax.all_gather(own, "fs", axis=0)
    own, got = lax.optimization_barrier((own, got))

    def restored(w):
        return (w.astype(F32) * (1.0 / UP)).astype(BF)

    own_1 = restored(own[:, :rows])
    sib_1 = lax.ppermute(own_1, "c", SWAP)
    width = peers * feats
    h, hd = call(
        functools.partial(first_half_kernel, hid),
        (jax.ShapeDtypeStruct((width, half), BF), jax.ShapeDtypeStruct((hid, half), BF)),
        (got, own_1),
        [pltpu.VMEM((peers, LANE), F32)],
        flops=4 * hid * width * half,
        limit=16 << 20,
    )
    own_2, h, hd = lax.optimization_barrier((own[:, rows:], h, hd))
    own_2 = restored(own_2)
    own_2, sib_1, h, hd = lax.optimization_barrier((own_2, sib_1, h, hd))
    step = call(
        functools.partial(second_half_kernel, hid),
        jax.ShapeDtypeStruct((SIDE, far, chip, half), BF),
        (got, h, hd, own_1, sib_1),
        [pltpu.VMEM((CORES * hid, half), BF)],
        flops=8 * hid * width * half,
        limit=16 << 20,
    )
    step = lax.all_to_all(step, "yl", 0, 0, tiled=True)
    size = far * chip
    step = call(scaled_kernel, jax.ShapeDtypeStruct((size + 16, half), F32), (step,))
    step = step.astype(jnp.float16)
    own_2, step = lax.optimization_barrier((own_2, step))
    sib_2 = lax.ppermute(own_2, "c", SWAP)
    shares = lax.all_gather(step, ("yh", "yl"), axis=0)
    factor = jnp.exp2(shares[:, size].astype(F32) - TOP)
    shares, factor = lax.optimization_barrier((shares, factor))
    sums = 0.0
    for k in range(far):
        part = slice(k * SIDE, (k + 1) * SIDE)
        sums = sums + shares[part, :size].astype(F32) * factor[part, None, :]
    sums = sums.reshape(SIDE, far, chip, half)
    step, middle, there = call(
        functools.partial(second_block_kernel, hid),
        (
            jax.ShapeDtypeStruct((SIDE, far, chip, half), BF),
            jax.ShapeDtypeStruct((chip, half), BF),
            jax.ShapeDtypeStruct((feats, half), BF),
        ),
        (sums, got, own_2, sib_2),
        [
            pltpu.VMEM((width, half), BF),
            pltpu.VMEM((width, half), BF),
            pltpu.VMEM((CORES * hid, half), BF),
            pltpu.VMEM((peers, LANE), F32),
        ],
        flops=12 * hid * width * half,
        limit=16 << 20,
    )
    other = lax.ppermute(there, "c", SWAP)
    step = lax.all_to_all(step, "yl", 0, 0, tiled=True)
    step = call(partial_kernel, jax.ShapeDtypeStruct(step.shape[1:], BF), (step,))
    step = step.reshape(far * CORES, feats, half)
    step = lax.all_to_all(step, ("yh", "c"), 0, 0, tiled=True)
    out = call(
        last_kernel, jax.ShapeDtypeStruct((feats, mine), BF), (step, got, middle, other)
    )
    return out.T


def solution(mesh):
    sizes = mesh.shape
    shape = (sizes["grp"], sizes["fs"], sizes["tp"] // CORES // SIDE, SIDE, CORES)
    wide = Mesh(mesh.devices.reshape(shape), ("grp", "fs", "yh", "yl", "c"))
    tp = ("yh", "yl", "c")
    block = (P(tp), P("fs", tp), P(tp), P("fs", tp), P(tp), P(tp, "fs"), P(tp))
    rows = P(("grp", "fs"), tp)
    return jax.shard_map(
        body, mesh=wide, in_specs=(rows, *block, *block), out_specs=rows, check_vma=False
    )
```

```python
import functools

import jax
import jax.numpy as jnp
from jax import lax
from jax.experimental import pallas as pl
from jax.experimental.pallas import tpu as pltpu
from jax.sharding import Mesh, PartitionSpec as P

epsilon = 1e-06
BF = jnp.bfloat16
F32 = jnp.float32
CORES = 2
SIDE = 4
LANE = 128
EXTRA = 32
TAIL = 8
UP = 2.0**18
TOP = 13.0
SWAP = [(0, 1), (1, 0)]
VMEM = pl.BlockSpec(memory_space=pltpu.VMEM)


def split3(v):
    hi = v.astype(BF).astype(F32)
    mid = (v - hi).astype(BF).astype(F32)
    return hi, mid, v - hi - mid


def chip_index():
    return lax.axis_index("yh") * SIDE + lax.axis_index("yl")


def seat(other):
    core = lax.axis_index("c")
    return chip_index() * CORES + (1 - core if other else core)


def wide_row(a):
    if a.shape[1] == LANE:
        return a
    fill = jnp.zeros((1, LANE - a.shape[1]), F32)
    return jnp.concatenate([a, fill], axis=1)


def prep_kernel(t_hbm, *refs):
    count = 8
    sources, out_ref = refs[:count], refs[count]
    t_ref, held, ext, sems = refs[count + 1], refs[count + 2 : 2 * count + 2], *refs[-2:]
    peers, rows, half = out_ref.shape
    feats = t_hbm.shape[0]
    copies = [pltpu.make_async_copy(t_hbm, t_ref, sems.at[count])]
    for k in range(count):
        copies.append(pltpu.make_async_copy(sources[k], held[k], sems.at[k]))
    for copy in copies:
        copy.start()
    ext[...] = jnp.zeros_like(ext)
    for copy in copies:
        copy.wait()
    vecs = [ref[...] for ref in held]
    for k in range(2):
        for p, (u, v) in enumerate(zip(split3(vecs[2 * k]), split3(vecs[2 * k + 1]))):
            ext[3 * k + p : 3 * k + p + 1, :] = wide_row(jnp.concatenate([u, v], axis=1))
    for j in range(4):
        for p, u in enumerate(split3(vecs[4 + j])):
            at = 8 + 8 * p + 2 * j
            ext[at : at + 1, :] = u[:, :LANE]
            ext[at + 1 : at + 2, :] = wide_row(u[:, LANE:])
    tail = ext[...].astype(BF)
    for k in range(peers):
        c = k % CORES
        out_ref[k, :feats, :] = t_ref[:, c * half : (c + 1) * half]
        out_ref[k, feats:, :] = tail


def vec_column(got, peer, which, feats, col, size):
    rows = got[peer, feats + 8 : feats + EXTRA, :].astype(F32)
    rows = rows[0:8] + rows[8:16] + rows[16:24]
    turned = jnp.transpose(rows)
    cols = []
    for w in which:
        a = turned[:, 2 * w : 2 * w + 1]
        b = turned[: size - LANE, 2 * w + 1 : 2 * w + 2]
        cols.append(jnp.concatenate([a, b], axis=0))
    return cols


def columns(got, rows, ref):
    feats = got.shape[1] - EXTRA
    for p in range(got.shape[0]):
        v = got[p, feats : feats + 8, :].astype(F32)
        ref[p : p + 1, :] = v[rows : rows + 1] + v[rows + 1 : rows + 2] + v[rows + 2 : rows + 3]
    return jnp.transpose(ref[...])


def normalize(block, piece, got, h_ref, g_ref):
    peers = got.shape[0]
    feats = got.shape[1] - EXTRA
    tokens = got.shape[2]
    width = feats * peers
    gains = columns(got, 0, g_ref)
    gains = gains[:feats] if block == 0 else gains[feats : 2 * feats]
    total = jnp.zeros((feats, tokens), F32)
    for p in range(peers):
        v = piece(p)
        total = total + v * v
    r = lax.rsqrt(jnp.sum(total, axis=0, keepdims=True) / float(width) + epsilon)
    for p in range(peers):
        h_ref[pl.ds(p * feats, feats), :] = (piece(p) * r * gains[:, p : p + 1]).astype(BF)


def hidden_of(hid, block, w, peer, got, h_ref):
    feats = got.shape[1] - EXTRA
    chunks, _, lane = w.shape
    sg, su = vec_column(got, peer, (2 * block, 2 * block + 1), feats, block, hid)
    acc = jnp.zeros((2 * hid, got.shape[2]), F32)
    for z in range(0, chunks, 2):
        lhs = jnp.concatenate([w[z, : 2 * hid, :], w[z + 1, : 2 * hid, :]], axis=1)
        acc = acc + jnp.dot(
            lhs, h_ref[pl.ds(z * lane, 2 * lane), :], preferred_element_type=F32
        )
    gate = acc[:hid] * sg
    up = acc[hid:] * su
    return (gate / (1.0 + jnp.exp(-gate)) * up).astype(BF)


def down_blocks(hid, own_ref, sib_ref, hidden, store):
    for z in range(own_ref.shape[0]):
        rows = slice(2 * hid, 3 * hid)
        lhs = jnp.concatenate([own_ref[z, rows, :], sib_ref[z, rows, :]], axis=0)
        part = lax.dot_general(
            lhs, hidden, (((0,), (0,)), ((), ())), preferred_element_type=F32
        )
        store(z, part.astype(BF))


def first_half_kernel(hid, got, own_ref, h_ref, hd_ref, g_ref):
    feats = got.shape[1] - EXTRA
    normalize(0, lambda p: got[p, :feats, :].astype(F32), got, h_ref, g_ref)
    hd_ref[...] = hidden_of(hid, 0, own_ref, seat(0), got, h_ref)


def second_half_kernel(hid, got, h_ref, hd_own, own_ref, sib_ref, out_ref, hd_ref):
    hd_ref[:hid, :] = hd_own[...]
    hd_ref[hid:, :] = hidden_of(hid, 0, sib_ref, seat(1), got, h_ref)

    def store(z, part):
        out_ref[z % SIDE, z // SIDE] = part

    down_blocks(hid, own_ref, sib_ref, hd_ref[...], store)


def second_block_kernel(
    hid, sums, got, own_ref, sib_ref, out_ref, mid_ref, there_ref, s_ref, h_ref, hd_ref, g_ref
):
    feats = got.shape[1] - EXTRA
    scales = columns(got, 3, g_ref)[:feats]
    for p in range(got.shape[0]):
        chip, c = divmod(p, CORES)
        part = sums[chip % SIDE, chip // SIDE, c * feats : (c + 1) * feats, :]
        mid = got[p, :feats, :].astype(F32) + 0.5 * part * scales[:, p : p + 1]
        s_ref[pl.ds(p * feats, feats), :] = mid.astype(BF)
    mine = chip_index() * CORES * feats
    mid_ref[...] = s_ref[pl.ds(mine, CORES * feats), :]
    there_ref[...] = s_ref[pl.ds(mine + (1 - lax.axis_index("c")) * feats, feats), :]
    normalize(1, lambda p: s_ref[pl.ds(p * feats, feats), :].astype(F32), got, h_ref, g_ref)
    hd_ref[:hid, :] = hidden_of(hid, 1, own_ref, seat(0), got, h_ref)
    hd_ref[hid:, :] = hidden_of(hid, 1, sib_ref, seat(1), got, h_ref)

    def store(z, part):
        out_ref[z % SIDE, z // SIDE] = part

    down_blocks(hid, own_ref, sib_ref, hd_ref[...], store)


def down_column(got, peer, block, feats):
    rows = got[peer, feats : feats + 8, :].astype(F32)
    row = rows[3:4] + rows[4:5] + rows[5:6]
    turned = jnp.transpose(jnp.broadcast_to(row, (8, LANE)))
    return turned[block * feats : (block + 1) * feats, 0:1]


def last_kernel(sums, got, mid_ref, other_ref, out_ref):
    feats = got.shape[1] - EXTRA
    half = got.shape[2]
    core = lax.axis_index("c")
    scale = down_column(got, seat(0), 1, feats)
    here = mid_ref[pl.ds(core * feats, feats), :].astype(F32)
    other = other_ref[...].astype(F32)
    for c in range(CORES):
        total = sums[c].astype(F32)
        for k in range(CORES + c, sums.shape[0], CORES):
            total = total + sums[k].astype(F32)
        resid = jnp.where(core == c, here, other)
        out_ref[:, c * half : (c + 1) * half] = (resid + 0.5 * total * scale).astype(BF)


def partial_kernel(got, out_ref):
    total = got[0].astype(F32)
    for k in range(1, got.shape[0]):
        total = total + got[k].astype(F32)
    out_ref[...] = total.astype(BF)


def scaled_kernel(got, out_ref):
    far, chip, _ = got.shape[1:]
    total = got[0].astype(F32)
    for k in range(1, got.shape[0]):
        total = total + got[k].astype(F32)
    top = jnp.max(jnp.max(jnp.abs(total), axis=0), axis=0, keepdims=True)
    top = jnp.maximum(top, 2.0**-100)
    power = jnp.clip(jnp.floor(jnp.log2(top)), -100.0, 120.0)
    factor = jnp.exp2(TOP - power)
    for i in range(far):
        out_ref[i * chip : (i + 1) * chip, :] = total[i] * factor
    tail = out_ref.shape[0] - far * chip
    out_ref[far * chip :, :] = jnp.broadcast_to(power, (tail, power.shape[1]))


def call(kernel, out, args, scratch=(), flops=1000, limit=4 << 20, space=pltpu.VMEM):
    specs = jax.tree.map(lambda _: VMEM, out)
    return pl.pallas_call(
        kernel,
        out_shape=out,
        in_specs=[pl.BlockSpec(memory_space=space)] * len(args),
        out_specs=specs,
        scratch_shapes=list(scratch),
        compiler_params=pltpu.CompilerParams(vmem_limit_bytes=limit),
        cost_estimate=pl.CostEstimate(flops=flops, bytes_accessed=1 << 20, transcendentals=0),
    )(*args)


def body(
    tokens,
    gain_1,
    gate_1,
    gate_s1,
    up_1,
    up_s1,
    down_1,
    down_s1,
    gain_2,
    gate_2,
    gate_s2,
    up_2,
    up_s2,
    down_2,
    down_s2,
):
    far = lax.axis_size("yh")
    peers = far * SIDE * CORES
    mine, feats = tokens.shape
    half = mine // CORES
    chip = feats * CORES
    hid = gate_1.shape[1]

    vecs = [v[None] for v in (gain_1, gain_2, down_s1, down_s2, gate_s1, up_s1, gate_s2, up_s2)]
    sent = call(
        prep_kernel,
        jax.ShapeDtypeStruct((peers, feats + EXTRA, half), BF),
        (tokens.T, *vecs),
        [
            pltpu.VMEM((feats, mine), BF),
            *(pltpu.VMEM(v.shape, F32) for v in vecs),
            pltpu.VMEM((EXTRA, LANE), F32),
            pltpu.SemaphoreType.DMA((len(vecs) + 1,)),
        ],
        limit=56 << 20,
        space=pltpu.HBM,
    )
    got = lax.all_to_all(sent, ("yh", "yl", "c"), 0, 0, tiled=True)

    rows = 3 * hid
    own = jnp.concatenate([gate_1.T, up_1.T, down_1, gate_2.T, up_2.T, down_2], axis=0)
    own = (own.astype(BF).astype(F32) * UP).astype(jnp.float16)
    own = lax.all_gather(own, "fs", axis=0)
    own, got = lax.optimization_barrier((own, got))

    def restored(w):
        return (w.astype(F32) * (1.0 / UP)).astype(BF)

    own_1 = restored(own[:, :rows])
    sib_1 = lax.ppermute(own_1, "c", SWAP)
    width = peers * feats
    h, hd = call(
        functools.partial(first_half_kernel, hid),
        (jax.ShapeDtypeStruct((width, half), BF), jax.ShapeDtypeStruct((hid, half), BF)),
        (got, own_1),
        [pltpu.VMEM((peers, LANE), F32)],
        flops=4 * hid * width * half,
        limit=16 << 20,
    )
    own_2, h, hd = lax.optimization_barrier((own[:, rows:], h, hd))
    own_2 = restored(own_2)
    own_2, sib_1, h, hd = lax.optimization_barrier((own_2, sib_1, h, hd))
    step = call(
        functools.partial(second_half_kernel, hid),
        jax.ShapeDtypeStruct((SIDE, far, chip, half), BF),
        (got, h, hd, own_1, sib_1),
        [pltpu.VMEM((CORES * hid, half), BF)],
        flops=8 * hid * width * half,
        limit=16 << 20,
    )
    step = lax.all_to_all(step, "yl", 0, 0, tiled=True)
    size = far * chip
    step = call(scaled_kernel, jax.ShapeDtypeStruct((size + TAIL, half), F32), (step,))
    step = step.astype(jnp.float16)
    own_2, step = lax.optimization_barrier((own_2, step))
    sib_2 = lax.ppermute(own_2, "c", SWAP)
    shares = lax.all_gather(step, ("yh", "yl"), axis=0)
    factor = jnp.exp2(shares[:, size].astype(F32) - TOP)
    shares, factor = lax.optimization_barrier((shares, factor))
    sums = 0.0
    for k in range(far):
        part = slice(k * SIDE, (k + 1) * SIDE)
        sums = sums + shares[part, :size].astype(F32) * factor[part, None, :]
    sums = sums.reshape(SIDE, far, chip, half)
    step, middle, there = call(
        functools.partial(second_block_kernel, hid),
        (
            jax.ShapeDtypeStruct((SIDE, far, chip, half), BF),
            jax.ShapeDtypeStruct((chip, half), BF),
            jax.ShapeDtypeStruct((feats, half), BF),
        ),
        (sums, got, own_2, sib_2),
        [
            pltpu.VMEM((width, half), BF),
            pltpu.VMEM((width, half), BF),
            pltpu.VMEM((CORES * hid, half), BF),
            pltpu.VMEM((peers, LANE), F32),
        ],
        flops=12 * hid * width * half,
        limit=16 << 20,
    )
    other = lax.ppermute(there, "c", SWAP)
    step = lax.all_to_all(step, "yl", 0, 0, tiled=True)
    step = call(partial_kernel, jax.ShapeDtypeStruct(step.shape[1:], BF), (step,))
    step = step.reshape(far * CORES, feats, half)
    step = lax.all_to_all(step, ("yh", "c"), 0, 0, tiled=True)
    out = call(
        last_kernel, jax.ShapeDtypeStruct((feats, mine), BF), (step, got, middle, other)
    )
    return out.T


def solution(mesh):
    sizes = mesh.shape
    shape = (sizes["grp"], sizes["fs"], sizes["tp"] // CORES // SIDE, SIDE, CORES)
    wide = Mesh(mesh.devices.reshape(shape), ("grp", "fs", "yh", "yl", "c"))
    tp = ("yh", "yl", "c")
    block = (P(tp), P("fs", tp), P(tp), P("fs", tp), P(tp), P(tp, "fs"), P(tp))
    rows = P(("grp", "fs"), tp)
    return jax.shard_map(
        body, mesh=wide, in_specs=(rows, *block, *block), out_specs=rows, check_vma=False
    )
```

```python
import functools

import jax
import jax.numpy as jnp
from jax import lax
from jax.experimental import pallas as pl
from jax.experimental.pallas import tpu as pltpu
from jax.sharding import Mesh, PartitionSpec as P

epsilon = 1e-06
BF = jnp.bfloat16
F32 = jnp.float32
CORES = 2
SIDE = 4
LANE = 128
EXTRA = 32
TAIL = 8
UP = 2.0**18
TOP = 13.0
SWAP = [(0, 1), (1, 0)]
VMEM = pl.BlockSpec(memory_space=pltpu.VMEM)


def split3(v):
    hi = v.astype(BF).astype(F32)
    mid = (v - hi).astype(BF).astype(F32)
    return hi, mid, v - hi - mid


def chip_index():
    return lax.axis_index("yh") * SIDE + lax.axis_index("yl")


def seat(got, other):
    core = lax.axis_index("c")
    return got.shape[0] - 1 - chip_index() * CORES - (1 - core if other else core)


def wide_row(a):
    if a.shape[1] == LANE:
        return a
    fill = jnp.zeros((1, LANE - a.shape[1]), F32)
    return jnp.concatenate([a, fill], axis=1)


def prep_kernel(t_hbm, *refs):
    count = 8
    sources, out_ref = refs[:count], refs[count]
    t_ref, held, ext, sems = refs[count + 1], refs[count + 2 : 2 * count + 2], *refs[-2:]
    peers, rows, half = out_ref.shape
    feats = t_hbm.shape[0]
    copies = [pltpu.make_async_copy(t_hbm, t_ref, sems.at[count])]
    for k in range(count):
        copies.append(pltpu.make_async_copy(sources[k], held[k], sems.at[k]))
    for copy in copies:
        copy.start()
    ext[...] = jnp.zeros_like(ext)
    for copy in copies:
        copy.wait()
    vecs = [ref[...] for ref in held]
    for k in range(2):
        for p, (u, v) in enumerate(zip(split3(vecs[2 * k]), split3(vecs[2 * k + 1]))):
            ext[3 * k + p : 3 * k + p + 1, :] = wide_row(jnp.concatenate([u, v], axis=1))
    for j in range(4):
        for p, u in enumerate(split3(vecs[4 + j])):
            at = 8 + 8 * p + 2 * j
            ext[at : at + 1, :] = u[:, :LANE]
            ext[at + 1 : at + 2, :] = wide_row(u[:, LANE:])
    tail = ext[...].astype(BF)
    for k in range(peers):
        c = (peers - 1 - k) % CORES
        out_ref[k, :feats, :] = t_ref[:, c * half : (c + 1) * half]
        out_ref[k, feats:, :] = tail


def vec_column(got, peer, which, feats, col, size):
    rows = got[peer, feats + 8 : feats + EXTRA, :].astype(F32)
    rows = rows[0:8] + rows[8:16] + rows[16:24]
    turned = jnp.transpose(rows)
    cols = []
    for w in which:
        a = turned[:, 2 * w : 2 * w + 1]
        b = turned[: size - LANE, 2 * w + 1 : 2 * w + 2]
        cols.append(jnp.concatenate([a, b], axis=0))
    return cols


def columns(got, rows, ref):
    feats = got.shape[1] - EXTRA
    for p in range(got.shape[0]):
        v = got[got.shape[0] - 1 - p, feats : feats + 8, :].astype(F32)
        ref[p : p + 1, :] = v[rows : rows + 1] + v[rows + 1 : rows + 2] + v[rows + 2 : rows + 3]
    return jnp.transpose(ref[...])


def normalize(block, piece, got, h_ref, g_ref):
    peers = got.shape[0]
    feats = got.shape[1] - EXTRA
    tokens = got.shape[2]
    width = feats * peers
    gains = columns(got, 0, g_ref)
    gains = gains[:feats] if block == 0 else gains[feats : 2 * feats]
    total = jnp.zeros((feats, tokens), F32)
    for p in range(peers):
        v = piece(p)
        total = total + v * v
    r = lax.rsqrt(jnp.sum(total, axis=0, keepdims=True) / float(width) + epsilon)
    for p in range(peers):
        h_ref[pl.ds(p * feats, feats), :] = (piece(p) * r * gains[:, p : p + 1]).astype(BF)


def hidden_of(hid, block, w, peer, got, h_ref):
    feats = got.shape[1] - EXTRA
    chunks, _, lane = w.shape
    sg, su = vec_column(got, peer, (2 * block, 2 * block + 1), feats, block, hid)
    acc = jnp.zeros((2 * hid, got.shape[2]), F32)
    for z in range(0, chunks, 2):
        lhs = jnp.concatenate([w[z, : 2 * hid, :], w[z + 1, : 2 * hid, :]], axis=1)
        acc = acc + jnp.dot(
            lhs, h_ref[pl.ds(z * lane, 2 * lane), :], preferred_element_type=F32
        )
    gate = acc[:hid] * sg
    up = acc[hid:] * su
    return (gate / (1.0 + jnp.exp(-gate)) * up).astype(BF)


def down_blocks(hid, own_ref, sib_ref, hidden, store):
    for z in range(own_ref.shape[0]):
        rows = slice(2 * hid, 3 * hid)
        lhs = jnp.concatenate([own_ref[z, rows, :], sib_ref[z, rows, :]], axis=0)
        part = lax.dot_general(
            lhs, hidden, (((0,), (0,)), ((), ())), preferred_element_type=F32
        )
        store(z, part.astype(BF))


def first_half_kernel(hid, got, own_ref, h_ref, hd_ref, g_ref):
    feats = got.shape[1] - EXTRA
    last = got.shape[0] - 1
    normalize(0, lambda p: got[last - p, :feats, :].astype(F32), got, h_ref, g_ref)
    hd_ref[...] = hidden_of(hid, 0, own_ref, seat(got, 0), got, h_ref)


def second_half_kernel(hid, got, h_ref, hd_own, own_ref, sib_ref, out_ref, hd_ref):
    hd_ref[:hid, :] = hd_own[...]
    hd_ref[hid:, :] = hidden_of(hid, 0, sib_ref, seat(got, 1), got, h_ref)

    def store(z, part):
        out_ref[z % SIDE, z // SIDE] = part

    down_blocks(hid, own_ref, sib_ref, hd_ref[...], store)


def second_block_kernel(
    hid, sums, got, own_ref, sib_ref, out_ref, mid_ref, there_ref, s_ref, h_ref, hd_ref, g_ref
):
    feats = got.shape[1] - EXTRA
    scales = columns(got, 3, g_ref)[:feats]
    for p in range(got.shape[0]):
        chip, c = divmod(p, CORES)
        part = sums[chip % SIDE, chip // SIDE, c * feats : (c + 1) * feats, :]
        mid = got[got.shape[0] - 1 - p, :feats, :].astype(F32) + 0.5 * part * scales[:, p : p + 1]
        s_ref[pl.ds(p * feats, feats), :] = mid.astype(BF)
    mine = chip_index() * CORES * feats
    mid_ref[...] = s_ref[pl.ds(mine, CORES * feats), :]
    there_ref[...] = s_ref[pl.ds(mine + (1 - lax.axis_index("c")) * feats, feats), :]
    normalize(1, lambda p: s_ref[pl.ds(p * feats, feats), :].astype(F32), got, h_ref, g_ref)
    hd_ref[:hid, :] = hidden_of(hid, 1, own_ref, seat(got, 0), got, h_ref)
    hd_ref[hid:, :] = hidden_of(hid, 1, sib_ref, seat(got, 1), got, h_ref)

    def store(z, part):
        out_ref[z % SIDE, z // SIDE] = part

    down_blocks(hid, own_ref, sib_ref, hd_ref[...], store)


def down_column(got, peer, block, feats):
    rows = got[peer, feats : feats + 8, :].astype(F32)
    row = rows[3:4] + rows[4:5] + rows[5:6]
    turned = jnp.transpose(jnp.broadcast_to(row, (8, LANE)))
    return turned[block * feats : (block + 1) * feats, 0:1]


def last_kernel(sums, got, mid_ref, other_ref, out_ref):
    feats = got.shape[1] - EXTRA
    half = got.shape[2]
    core = lax.axis_index("c")
    scale = down_column(got, seat(got, 0), 1, feats)
    here = mid_ref[pl.ds(core * feats, feats), :].astype(F32)
    other = other_ref[...].astype(F32)
    for c in range(CORES):
        total = sums[c].astype(F32)
        for k in range(CORES + c, sums.shape[0], CORES):
            total = total + sums[k].astype(F32)
        resid = jnp.where(core == c, here, other)
        out_ref[:, c * half : (c + 1) * half] = (resid + 0.5 * total * scale).astype(BF)


def partial_kernel(got, out_ref):
    total = got[0].astype(F32)
    for k in range(1, got.shape[0]):
        total = total + got[k].astype(F32)
    out_ref[...] = total.astype(BF)


def scaled_kernel(got, out_ref):
    far, chip, _ = got.shape[1:]
    total = got[0].astype(F32)
    for k in range(1, got.shape[0]):
        total = total + got[k].astype(F32)
    top = jnp.max(jnp.max(jnp.abs(total), axis=0), axis=0, keepdims=True)
    top = jnp.maximum(top, 2.0**-100)
    power = jnp.clip(jnp.floor(jnp.log2(top)), -100.0, 120.0)
    factor = jnp.exp2(TOP - power)
    for i in range(far):
        out_ref[i * chip : (i + 1) * chip, :] = total[i] * factor
    tail = out_ref.shape[0] - far * chip
    out_ref[far * chip :, :] = jnp.broadcast_to(power, (tail, power.shape[1]))


def call(kernel, out, args, scratch=(), flops=1000, limit=4 << 20, space=pltpu.VMEM):
    specs = jax.tree.map(lambda _: VMEM, out)
    return pl.pallas_call(
        kernel,
        out_shape=out,
        in_specs=[pl.BlockSpec(memory_space=space)] * len(args),
        out_specs=specs,
        scratch_shapes=list(scratch),
        compiler_params=pltpu.CompilerParams(vmem_limit_bytes=limit),
        cost_estimate=pl.CostEstimate(flops=flops, bytes_accessed=1 << 20, transcendentals=0),
    )(*args)


def body(
    tokens,
    gain_1,
    gate_1,
    gate_s1,
    up_1,
    up_s1,
    down_1,
    down_s1,
    gain_2,
    gate_2,
    gate_s2,
    up_2,
    up_s2,
    down_2,
    down_s2,
):
    far = lax.axis_size("yh")
    peers = far * SIDE * CORES
    mine, feats = tokens.shape
    half = mine // CORES
    chip = feats * CORES
    hid = gate_1.shape[1]

    vecs = [v[None] for v in (gain_1, gain_2, down_s1, down_s2, gate_s1, up_s1, gate_s2, up_s2)]
    sent = call(
        prep_kernel,
        jax.ShapeDtypeStruct((peers, feats + EXTRA, half), BF),
        (tokens.T, *vecs),
        [
            pltpu.VMEM((feats, mine), BF),
            *(pltpu.VMEM(v.shape, F32) for v in vecs),
            pltpu.VMEM((EXTRA, LANE), F32),
            pltpu.SemaphoreType.DMA((len(vecs) + 1,)),
        ],
        limit=56 << 20,
        space=pltpu.HBM,
    )
    back = [list(range(peers - 1, -1, -1))]
    got = lax.all_to_all(
        sent, ("yh", "yl", "c"), 0, 0, tiled=True, axis_index_groups=back
    )

    rows = 3 * hid
    own = jnp.concatenate([gate_1.T, up_1.T, down_1, gate_2.T, up_2.T, down_2], axis=0)
    own = (own.astype(BF).astype(F32) * UP).astype(jnp.float16)
    own = lax.all_gather(own, "fs", axis=0)
    own, got = lax.optimization_barrier((own, got))

    def restored(w):
        return (w.astype(F32) * (1.0 / UP)).astype(BF)

    own_1 = restored(own[:, :rows])
    sib_1 = lax.ppermute(own_1, "c", SWAP)
    width = peers * feats
    h, hd = call(
        functools.partial(first_half_kernel, hid),
        (jax.ShapeDtypeStruct((width, half), BF), jax.ShapeDtypeStruct((hid, half), BF)),
        (got, own_1),
        [pltpu.VMEM((peers, LANE), F32)],
        flops=4 * hid * width * half,
        limit=16 << 20,
    )
    own_2, h, hd = lax.optimization_barrier((own[:, rows:], h, hd))
    own_2 = restored(own_2)
    own_2, sib_1, h, hd = lax.optimization_barrier((own_2, sib_1, h, hd))
    step = call(
        functools.partial(second_half_kernel, hid),
        jax.ShapeDtypeStruct((SIDE, far, chip, half), BF),
        (got, h, hd, own_1, sib_1),
        [pltpu.VMEM((CORES * hid, half), BF)],
        flops=8 * hid * width * half,
        limit=16 << 20,
    )
    step = lax.all_to_all(step, "yl", 0, 0, tiled=True)
    size = far * chip
    step = call(scaled_kernel, jax.ShapeDtypeStruct((size + TAIL, half), F32), (step,))
    step = step.astype(jnp.float16)
    own_2, step = lax.optimization_barrier((own_2, step))
    sib_2 = lax.ppermute(own_2, "c", SWAP)
    shares = lax.all_gather(step, ("yh", "yl"), axis=0)
    factor = jnp.exp2(shares[:, size].astype(F32) - TOP)
    shares, factor = lax.optimization_barrier((shares, factor))
    sums = 0.0
    for k in range(far):
        part = slice(k * SIDE, (k + 1) * SIDE)
        sums = sums + shares[part, :size].astype(F32) * factor[part, None, :]
    sums = sums.reshape(SIDE, far, chip, half)
    step, middle, there = call(
        functools.partial(second_block_kernel, hid),
        (
            jax.ShapeDtypeStruct((SIDE, far, chip, half), BF),
            jax.ShapeDtypeStruct((chip, half), BF),
            jax.ShapeDtypeStruct((feats, half), BF),
        ),
        (sums, got, own_2, sib_2),
        [
            pltpu.VMEM((width, half), BF),
            pltpu.VMEM((width, half), BF),
            pltpu.VMEM((CORES * hid, half), BF),
            pltpu.VMEM((peers, LANE), F32),
        ],
        flops=12 * hid * width * half,
        limit=16 << 20,
    )
    other = lax.ppermute(there, "c", SWAP)
    step = lax.all_to_all(step, "yl", 0, 0, tiled=True)
    step = call(partial_kernel, jax.ShapeDtypeStruct(step.shape[1:], BF), (step,))
    step = step.reshape(far * CORES, feats, half)
    step = lax.all_to_all(step, ("yh", "c"), 0, 0, tiled=True)
    out = call(
        last_kernel, jax.ShapeDtypeStruct((feats, mine), BF), (step, got, middle, other)
    )
    return out.T


def solution(mesh):
    sizes = mesh.shape
    shape = (sizes["grp"], sizes["fs"], sizes["tp"] // CORES // SIDE, SIDE, CORES)
    wide = Mesh(mesh.devices.reshape(shape), ("grp", "fs", "yh", "yl", "c"))
    tp = ("yh", "yl", "c")
    block = (P(tp), P("fs", tp), P(tp), P("fs", tp), P(tp), P(tp, "fs"), P(tp))
    rows = P(("grp", "fs"), tp)
    return jax.shard_map(
        body, mesh=wide, in_specs=(rows, *block, *block), out_specs=rows, check_vma=False
    )
```

```python
import functools

import jax
import jax.numpy as jnp
from jax import lax
from jax.experimental import pallas as pl
from jax.experimental.pallas import tpu as pltpu
from jax.sharding import Mesh, PartitionSpec as P


epsilon = 1e-06
BF = jnp.bfloat16
F32 = jnp.float32
CORES = 2
SIDE = 4
LANE = 128
EXTRA = 32
TAIL = 8
UP = 2.0**18
TOP = 13.0
SWAP = [(0, 1), (1, 0)]
VMEM = pl.BlockSpec(memory_space=pltpu.VMEM)


def split3(v):
    hi = v.astype(BF).astype(F32)
    mid = (v - hi).astype(BF).astype(F32)
    return hi, mid, v - hi - mid


def chip_index():
    return lax.axis_index("yh") * SIDE + lax.axis_index("yl")


def seat(got, other):
    core = lax.axis_index("c")
    return got.shape[0] - 1 - chip_index() * CORES - (1 - core if other else core)


def wide_row(a):
    if a.shape[1] == LANE:
        return a
    fill = jnp.zeros((1, LANE - a.shape[1]), F32)
    return jnp.concatenate([a, fill], axis=1)


def prep_kernel(t_hbm, *refs):
    count = 8
    sources, out_ref = refs[:count], refs[count]
    t_ref, held, ext, sems = refs[count + 1], refs[count + 2 : 2 * count + 2], *refs[-2:]
    peers, _, half = out_ref.shape
    feats = t_hbm.shape[0]
    copies = [pltpu.make_async_copy(t_hbm, t_ref, sems.at[count])]
    for k in range(count):
        copies.append(pltpu.make_async_copy(sources[k], held[k], sems.at[k]))
    for copy in copies:
        copy.start()
    ext[...] = jnp.zeros_like(ext)
    for copy in copies:
        copy.wait()
    vecs = [ref[...] for ref in held]
    for k in range(2):
        for p, (u, v) in enumerate(zip(split3(vecs[2 * k]), split3(vecs[2 * k + 1]))):
            ext[3 * k + p : 3 * k + p + 1, :] = wide_row(jnp.concatenate([u, v], axis=1))
    for j in range(4):
        for p, u in enumerate(split3(vecs[4 + j])):
            at = 8 + 8 * p + 2 * j
            ext[at : at + 1, :] = u[:, :LANE]
            ext[at + 1 : at + 2, :] = wide_row(u[:, LANE:])
    tail = ext[...].astype(BF)
    for k in range(peers):
        c = (peers - 1 - k) % CORES
        out_ref[k, :feats, :] = t_ref[:, c * half : (c + 1) * half]
        out_ref[k, feats:, :] = tail


def vec_column(got, peer, which, feats, size):
    rows = got[peer, feats + 8 : feats + EXTRA, :].astype(F32)
    rows = rows[0:8] + rows[8:16] + rows[16:24]
    turned = jnp.transpose(rows)
    cols = []
    for w in which:
        a = turned[:, 2 * w : 2 * w + 1]
        b = turned[: size - LANE, 2 * w + 1 : 2 * w + 2]
        cols.append(jnp.concatenate([a, b], axis=0))
    return cols


def columns(got, rows, ref):
    feats = got.shape[1] - EXTRA
    for p in range(got.shape[0]):
        v = got[got.shape[0] - 1 - p, feats : feats + 8, :].astype(F32)
        ref[p : p + 1, :] = v[rows : rows + 1] + v[rows + 1 : rows + 2] + v[rows + 2 : rows + 3]
    return jnp.transpose(ref[...])


def normalize(block, piece, got, h_ref, g_ref):
    peers = got.shape[0]
    feats = got.shape[1] - EXTRA
    tokens = got.shape[2]
    width = feats * peers
    gains = columns(got, 0, g_ref)
    gains = gains[:feats] if block == 0 else gains[feats : 2 * feats]
    total = jnp.zeros((feats, tokens), F32)
    for p in range(peers):
        v = piece(p)
        total = total + v * v
    r = lax.rsqrt(jnp.sum(total, axis=0, keepdims=True) / float(width) + epsilon)
    for p in range(peers):
        h_ref[pl.ds(p * feats, feats), :] = (piece(p) * r * gains[:, p : p + 1]).astype(BF)


def hidden_of(hid, block, w, peer, got, h_ref):
    feats = got.shape[1] - EXTRA
    chunks, _, lane = w.shape
    sg, su = vec_column(got, peer, (2 * block, 2 * block + 1), feats, hid)
    acc = jnp.zeros((2 * hid, got.shape[2]), F32)
    for z in range(0, chunks, 2):
        lhs = jnp.concatenate([w[z, : 2 * hid, :], w[z + 1, : 2 * hid, :]], axis=1)
        acc = acc + jnp.dot(
            lhs, h_ref[pl.ds(z * lane, 2 * lane), :], preferred_element_type=F32
        )
    gate = acc[:hid] * sg
    up = acc[hid:] * su
    return (gate / (1.0 + jnp.exp(-gate)) * up).astype(BF)


def down_blocks(hid, own_ref, sib_ref, hidden, store):
    for z in range(own_ref.shape[0]):
        rows = slice(2 * hid, 3 * hid)
        lhs = jnp.concatenate([own_ref[z, rows, :], sib_ref[z, rows, :]], axis=0)
        part = lax.dot_general(
            lhs, hidden, (((0,), (0,)), ((), ())), preferred_element_type=F32
        )
        store(z, part.astype(BF))


def first_half_kernel(hid, got, own_ref, h_ref, hd_ref, g_ref):
    feats = got.shape[1] - EXTRA
    last = got.shape[0] - 1
    normalize(0, lambda p: got[last - p, :feats, :].astype(F32), got, h_ref, g_ref)
    hd_ref[...] = hidden_of(hid, 0, own_ref, seat(got, 0), got, h_ref)


def second_half_kernel(hid, got, h_ref, hd_own, own_ref, sib_ref, out_ref, hd_ref):
    hd_ref[:hid, :] = hd_own[...]
    hd_ref[hid:, :] = hidden_of(hid, 0, sib_ref, seat(got, 1), got, h_ref)

    def store(z, part):
        out_ref[z % SIDE, z // SIDE] = part

    down_blocks(hid, own_ref, sib_ref, hd_ref[...], store)


def second_block_kernel(
    hid, sums, got, own_ref, sib_ref, out_ref, mid_ref, there_ref, s_ref, h_ref, hd_ref, g_ref
):
    feats = got.shape[1] - EXTRA
    scales = columns(got, 3, g_ref)[:feats]
    for p in range(got.shape[0]):
        chip, c = divmod(p, CORES)
        part = sums[chip % SIDE, chip // SIDE, c * feats : (c + 1) * feats, :]
        mid = got[got.shape[0] - 1 - p, :feats, :].astype(F32) + 0.5 * part * scales[:, p : p + 1]
        s_ref[pl.ds(p * feats, feats), :] = mid.astype(BF)
    mine = chip_index() * CORES * feats
    mid_ref[...] = s_ref[pl.ds(mine, CORES * feats), :]
    there_ref[...] = s_ref[pl.ds(mine + (1 - lax.axis_index("c")) * feats, feats), :]
    normalize(1, lambda p: s_ref[pl.ds(p * feats, feats), :].astype(F32), got, h_ref, g_ref)
    hd_ref[:hid, :] = hidden_of(hid, 1, own_ref, seat(got, 0), got, h_ref)
    hd_ref[hid:, :] = hidden_of(hid, 1, sib_ref, seat(got, 1), got, h_ref)

    def store(z, part):
        out_ref[z % SIDE, z // SIDE] = part

    down_blocks(hid, own_ref, sib_ref, hd_ref[...], store)


def down_column(got, peer, block, feats):
    rows = got[peer, feats : feats + 8, :].astype(F32)
    row = rows[3:4] + rows[4:5] + rows[5:6]
    turned = jnp.transpose(jnp.broadcast_to(row, (8, LANE)))
    return turned[block * feats : (block + 1) * feats, 0:1]


def last_kernel(sums, got, mid_ref, other_ref, out_ref):
    feats = got.shape[1] - EXTRA
    half = got.shape[2]
    core = lax.axis_index("c")
    scale = down_column(got, seat(got, 0), 1, feats)
    here = mid_ref[pl.ds(core * feats, feats), :].astype(F32)
    other = other_ref[...].astype(F32)
    for c in range(CORES):
        total = sums[c].astype(F32)
        for k in range(CORES + c, sums.shape[0], CORES):
            total = total + sums[k].astype(F32)
        resid = jnp.where(core == c, here, other)
        out_ref[:, c * half : (c + 1) * half] = (resid + 0.5 * total * scale).astype(BF)


def partial_kernel(got, out_ref):
    total = got[0].astype(F32)
    for k in range(1, got.shape[0]):
        total = total + got[k].astype(F32)
    out_ref[...] = total.astype(BF)


def scaled_kernel(got, out_ref):
    far, chip, _ = got.shape[1:]
    total = got[0].astype(F32)
    for k in range(1, got.shape[0]):
        total = total + got[k].astype(F32)
    top = jnp.max(jnp.max(jnp.abs(total), axis=0), axis=0, keepdims=True)
    top = jnp.maximum(top, 2.0**-100)
    power = jnp.clip(jnp.floor(jnp.log2(top)), -100.0, 120.0)
    factor = jnp.exp2(TOP - power)
    for i in range(far):
        out_ref[i * chip : (i + 1) * chip, :] = total[i] * factor
    tail = out_ref.shape[0] - far * chip
    out_ref[far * chip :, :] = jnp.broadcast_to(power, (tail, power.shape[1]))


def call(kernel, out, args, scratch=(), flops=1000, limit=4 << 20, space=pltpu.VMEM):
    specs = jax.tree.map(lambda _: VMEM, out)
    return pl.pallas_call(
        kernel,
        out_shape=out,
        in_specs=[pl.BlockSpec(memory_space=space)] * len(args),
        out_specs=specs,
        scratch_shapes=list(scratch),
        compiler_params=pltpu.CompilerParams(vmem_limit_bytes=limit),
        cost_estimate=pl.CostEstimate(flops=flops, bytes_accessed=1 << 20, transcendentals=0),
    )(*args)


def blocks(
    tokens,
    gain_1,
    gate_1,
    gate_s1,
    up_1,
    up_s1,
    down_1,
    down_s1,
    gain_2,
    gate_2,
    gate_s2,
    up_2,
    up_s2,
    down_2,
    down_s2,
):
    far = lax.axis_size("yh")
    peers = far * SIDE * CORES
    mine, feats = tokens.shape
    half = mine // CORES
    chip = feats * CORES
    hid = gate_1.shape[1]

    vecs = [v[None] for v in (gain_1, gain_2, down_s1, down_s2, gate_s1, up_s1, gate_s2, up_s2)]
    sent = call(
        prep_kernel,
        jax.ShapeDtypeStruct((peers, feats + EXTRA, half), BF),
        (tokens.T, *vecs),
        [
            pltpu.VMEM((feats, mine), BF),
            *(pltpu.VMEM(v.shape, F32) for v in vecs),
            pltpu.VMEM((EXTRA, LANE), F32),
            pltpu.SemaphoreType.DMA((len(vecs) + 1,)),
        ],
        limit=56 << 20,
        space=pltpu.HBM,
    )
    back = [list(range(peers - 1, -1, -1))]
    got = lax.all_to_all(
        sent, ("yh", "yl", "c"), 0, 0, tiled=True, axis_index_groups=back
    )

    rows = 3 * hid
    own = jnp.concatenate([gate_1.T, up_1.T, down_1, gate_2.T, up_2.T, down_2], axis=0)
    own = (own.astype(BF).astype(F32) * UP).astype(jnp.float16)
    own = lax.all_gather(own, "fs", axis=0)
    own, got = lax.optimization_barrier((own, got))

    def restored(w):
        return (w.astype(F32) * (1.0 / UP)).astype(BF)

    own_1 = restored(own[:, :rows])
    sib_1 = lax.ppermute(own_1, "c", SWAP)
    width = peers * feats
    h, hd = call(
        functools.partial(first_half_kernel, hid),
        (jax.ShapeDtypeStruct((width, half), BF), jax.ShapeDtypeStruct((hid, half), BF)),
        (got, own_1),
        [pltpu.VMEM((peers, LANE), F32)],
        flops=4 * hid * width * half,
        limit=16 << 20,
    )
    own_2, h, hd = lax.optimization_barrier((own[:, rows:], h, hd))
    own_2 = restored(own_2)
    sib_2 = lax.ppermute(own_2, "c", SWAP)
    own_2, sib_1, h, hd = lax.optimization_barrier((own_2, sib_1, h, hd))
    step = call(
        functools.partial(second_half_kernel, hid),
        jax.ShapeDtypeStruct((SIDE, far, chip, half), BF),
        (got, h, hd, own_1, sib_1),
        [pltpu.VMEM((CORES * hid, half), BF)],
        flops=8 * hid * width * half,
        limit=16 << 20,
    )
    step = lax.all_to_all(step, "yl", 0, 0, tiled=True)
    size = far * chip
    step = call(scaled_kernel, jax.ShapeDtypeStruct((size + TAIL, half), F32), (step,))
    step = step.astype(jnp.float16)
    shares = lax.all_gather(step, ("yh", "yl"), axis=0)
    factor = jnp.exp2(shares[:, size].astype(F32) - TOP)
    shares, factor = lax.optimization_barrier((shares, factor))
    sums = 0.0
    for k in range(far):
        part = slice(k * SIDE, (k + 1) * SIDE)
        sums = sums + shares[part, :size].astype(F32) * factor[part, None, :]
    sums = sums.reshape(SIDE, far, chip, half)
    step, middle, there = call(
        functools.partial(second_block_kernel, hid),
        (
            jax.ShapeDtypeStruct((SIDE, far, chip, half), BF),
            jax.ShapeDtypeStruct((chip, half), BF),
            jax.ShapeDtypeStruct((feats, half), BF),
        ),
        (sums, got, own_2, sib_2),
        [
            pltpu.VMEM((width, half), BF),
            pltpu.VMEM((width, half), BF),
            pltpu.VMEM((CORES * hid, half), BF),
            pltpu.VMEM((peers, LANE), F32),
        ],
        flops=12 * hid * width * half,
        limit=16 << 20,
    )
    other = lax.ppermute(there, "c", SWAP)
    step = lax.all_to_all(step, "yl", 0, 0, tiled=True)
    step = call(partial_kernel, jax.ShapeDtypeStruct(step.shape[1:], BF), (step,))
    step = step.reshape(far * CORES, feats, half)
    step = lax.all_to_all(step, ("yh", "c"), 0, 0, tiled=True)
    out = call(
        last_kernel, jax.ShapeDtypeStruct((feats, mine), BF), (step, got, middle, other)
    )
    return out.T


def solution(mesh):
    sizes = mesh.shape
    shape = (sizes["grp"], sizes["fs"], sizes["tp"] // CORES // SIDE, SIDE, CORES)
    wide = Mesh(mesh.devices.reshape(shape), ("grp", "fs", "yh", "yl", "c"))
    tp = ("yh", "yl", "c")
    block = (P(tp), P("fs", tp), P(tp), P("fs", tp), P(tp), P(tp, "fs"), P(tp))
    rows = P(("grp", "fs"), tp)
    return jax.shard_map(
        blocks, mesh=wide, in_specs=(rows, *block, *block), out_specs=rows, check_vma=False
    )
```
